32 devices in a mesh: fs: 8 (over z, x), tp: 4 (over y, core).
Axes of the slice: x: 2, y: 2, z: 4, core: 2. Of those that a mesh axis runs over, the one named last changes fastest.
Arguments:
- tokens: bfloat16 [6144, 2048], P('fs', 'tp'), may hold values from -6 to 6
- ffn_one_gain: float32 [2048], replicated, may hold values from 0.1 to 1.9
- ffn_one_gate: bfloat16 [2048, 5632], P('fs', 'tp'), may hold values from -0.125 to 0.125
- ffn_one_up: bfloat16 [2048, 5632], P('fs', 'tp'), may hold values from -0.125 to 0.125
- ffn_one_down: bfloat16 [5632, 2048], P('tp', 'fs'), may hold values from -0.078125 to 0.078125
- mix_gain: float32 [2048], replicated, may hold values from 0.1 to 1.9
- conv_value: bfloat16 [2048, 1024], P('fs', 'tp'), may hold values from -0.125 to 0.125
- conv_gate: bfloat16 [2048, 1024], P('fs', 'tp'), may hold values from -0.125 to 0.125
- conv_kernel: float32 [31, 1024], P(None, 'tp'), may hold values from -15 to 15
- conv_ln_gain: float32 [1024], P('tp'), may hold values from 0.1 to 1.9
- conv_out: bfloat16 [1024, 2048], P('tp', 'fs'), may hold values from -0.1875 to 0.1875
- ffn_two_gain: float32 [2048], replicated, may hold values from 0.1 to 1.9
- ffn_two_gate: bfloat16 [2048, 5632], P('fs', 'tp'), may hold values from -0.125 to 0.125
- ffn_two_up: bfloat16 [2048, 5632], P('fs', 'tp'), may hold values from -0.125 to 0.125
- ffn_two_down: bfloat16 [5632, 2048], P('tp', 'fs'), may hold values from -0.078125 to 0.078125
Outputs:
- layer_out: bfloat16 [6144, 2048], P('fs', 'tp')
The draws below stay inside these ranges and needn't reach their ends.
All inputs are finite; a program needn't handle non-finite values.
Results may differ from the reference program's by a relative error of at most 0.017.
Values may be sent and summed in bfloat16 or wider, within the bound.
No kernel may reach another device: no remote copies, remote signals or barrier semaphores. Data moves between devices by JAX's collectives and lax.ppermute only.
A program may use at most 128 MiB of HBM per device.

```python
import jax
import jax.numpy as jnp
from jax import lax

D = 2048
FF = 5632
CONV = 1024
KW = 31
TOK_DEV = 768
TOKENS = 6144
N_FS = 8
N_TP = 4


def draw_conv_kernel(key, part):
    first_key, second_key = jax.random.split(jax.random.fold_in(key, 7))
    base = jnp.clip(jax.random.normal(first_key, (KW, CONV), jnp.float32), -4.0, 4.0) / jnp.sqrt(jnp.float32(KW))
    position = jnp.arange(CONV, dtype=jnp.float32) / jnp.float32(max(CONV - 1, 1))
    rising = 3.0 ** position * jax.random.uniform(second_key, (CONV,), jnp.float32, 0.7, 1.4)
    return base * rising[None, :]


def shard_levels(key, extent, cuts, least, high):
    factor_of, own = 1.0, jax.random.fold_in(key, 6)
    for dim, shards_of in cuts:
        heights = jnp.exp(jax.random.uniform(jax.random.fold_in(own, dim), (shards_of,), jnp.float32, least / len(cuts), high / len(cuts)))
        factor_of = factor_of * jnp.repeat(heights, extent[dim] // shards_of).reshape([-1 if axis == dim else 1 for axis in range(len(extent))])
    return factor_of


def scatter_about(stream_key, dims, width, bound, shards=(), held_as=jnp.bfloat16):
    entries = jax.random.normal(stream_key, dims, jnp.float32) * width
    if len(shards) > 0:
        entries = shard_levels(stream_key, dims, shards, -0.22, 0.18) * entries
    return jnp.clip(entries, min=-bound, max=bound).astype(held_as)


def setup_inputs(seed: int = 0) -> dict:
    key_of = jax.random.split(jax.random.key(seed), 16)
    tokens = scatter_about(key_of[0], (TOKENS, D), 1.0, 6.0, ((0, 8), (1, 4)))
    ffn_one_gain = jnp.clip(1.0 + 0.18 * jax.random.normal(key_of[1], (D,), jnp.float32), 0.1, 1.9)
    ffn_one_gate = scatter_about(key_of[2], (D, FF), D ** -0.5, 0.125, ((0, 8), (1, 4)))
    ffn_one_up = scatter_about(key_of[3], (D, FF), D ** -0.5, 0.125, ((0, 8), (1, 4)))
    ffn_one_down = scatter_about(key_of[4], (FF, D), FF ** -0.5, 0.078125, ((0, 4), (1, 8)))
    mix_gain = jnp.clip(1.0 + 0.18 * jax.random.normal(key_of[5], (D,), jnp.float32), 0.1, 1.9)
    conv_value = scatter_about(key_of[6], (D, CONV), D ** -0.5, 0.125, ((0, 8), (1, 4)))
    conv_gate = scatter_about(key_of[7], (D, CONV), D ** -0.5, 0.125, ((0, 8), (1, 4)))
    conv_kernel = draw_conv_kernel(jax.random.fold_in(key_of[15], 71), 0)
    conv_ln_gain = jnp.clip(1.0 + 0.18 * jax.random.normal(key_of[9], (CONV,), jnp.float32), 0.1, 1.9)
    conv_out = scatter_about(key_of[10], (CONV, D), CONV ** -0.5, 0.1875, ((0, 4), (1, 8)))
    ffn_two_gain = jnp.clip(1.0 + 0.18 * jax.random.normal(key_of[11], (D,), jnp.float32), 0.1, 1.9)
    ffn_two_gate = scatter_about(key_of[12], (D, FF), D ** -0.5, 0.125, ((0, 8), (1, 4)))
    ffn_two_up = scatter_about(key_of[13], (D, FF), D ** -0.5, 0.125, ((0, 8), (1, 4)))
    ffn_two_down = scatter_about(key_of[14], (FF, D), FF ** -0.5, 0.078125, ((0, 4), (1, 8)))
    return dict(tokens=tokens, ffn_one_gain=ffn_one_gain, ffn_one_gate=ffn_one_gate, ffn_one_up=ffn_one_up, ffn_one_down=ffn_one_down, mix_gain=mix_gain, conv_value=conv_value, conv_gate=conv_gate, conv_kernel=conv_kernel, conv_ln_gain=conv_ln_gain, conv_out=conv_out, ffn_two_gain=ffn_two_gain, ffn_two_gate=ffn_two_gate, ffn_two_up=ffn_two_up, ffn_two_down=ffn_two_down)


def rms_rows(rows_in, gain_vec):
    values = rows_in.astype(jnp.float32)
    scaled = values * lax.rsqrt(lax.optimization_barrier(jnp.mean(values * values, axis=-1, keepdims=True)) + 1e-06) * gain_vec
    return scaled.astype(jnp.bfloat16)

def block_sum(hidden, weight, blocks):
    span_width = hidden.shape[1] // blocks
    summed = jnp.zeros((hidden.shape[0], weight.shape[1]), jnp.float32)
    for block_index in range(blocks):
        lower = block_index * span_width
        partial_value = jnp.dot(hidden[:, lower:lower + span_width], weight[lower:lower + span_width], preferred_element_type=jnp.float32).astype(jnp.bfloat16)
        summed = summed + lax.optimization_barrier(partial_value).astype(jnp.float32)
    return summed

def half_ffn(residual, gain_vec, w_gate, w_up, w_down):
    normed = rms_rows(residual, gain_vec)
    gate_pre = jnp.dot(normed, w_gate, preferred_element_type=jnp.float32)
    up_pre = jnp.dot(normed, w_up, preferred_element_type=jnp.float32)
    hidden = (jax.nn.silu(gate_pre) * up_pre).astype(jnp.bfloat16)
    summed = block_sum(hidden, w_down, N_TP)
    return (residual.astype(jnp.float32) + 0.5 * summed).astype(jnp.bfloat16)

def conv_module(residual, mix_gain, conv_value, conv_gate, conv_kernel, conv_ln_gain, conv_out):
    normed = rms_rows(residual, mix_gain)
    value_pre = jnp.dot(normed, conv_value, preferred_element_type=jnp.float32)
    gate_pre = jnp.dot(normed, conv_gate, preferred_element_type=jnp.float32)
    gated_lin = value_pre * jax.nn.sigmoid(gate_pre)
    sequences = gated_lin.reshape(N_FS, TOK_DEV, CONV)
    half_span = KW // 2
    convolved = lax.conv_general_dilated(sequences, conv_kernel[:, None, :], (1,), [(half_span, half_span)], dimension_numbers=('NWC', 'WIO', 'NWC'), feature_group_count=CONV, precision=lax.Precision.HIGHEST).reshape(N_FS * TOK_DEV, CONV)
    mean_val = lax.optimization_barrier(jnp.sum(convolved, axis=1, keepdims=True)) / CONV
    sq_mean = lax.optimization_barrier(jnp.sum(convolved * convolved, axis=1, keepdims=True)) / CONV
    varied = sq_mean - mean_val * mean_val
    active = jax.nn.silu((convolved - mean_val) * lax.rsqrt(varied + 1e-05) * conv_ln_gain).astype(jnp.bfloat16)
    summed = block_sum(active, conv_out, N_TP)
    return (residual.astype(jnp.float32) + summed).astype(jnp.bfloat16)

def reference(tokens, ffn_one_gain, ffn_one_gate, ffn_one_up, ffn_one_down, mix_gain, conv_value, conv_gate, conv_kernel, conv_ln_gain, conv_out, ffn_two_gain, ffn_two_gate, ffn_two_up, ffn_two_down):
    stream = half_ffn(tokens, ffn_one_gain, ffn_one_gate, ffn_one_up, ffn_one_down)
    stream = conv_module(stream, mix_gain, conv_value, conv_gate, conv_kernel, conv_ln_gain, conv_out)
    return half_ffn(stream, ffn_two_gain, ffn_two_gate, ffn_two_up, ffn_two_down)
```

```python
import jax
import jax.numpy as jnp
import numpy as np
from jax import lax
from jax.sharding import PartitionSpec as P


def spots_of(devices):
    return [tuple(getattr(device, "coords", (0, 0, place))) for place, device in enumerate(devices)]


def grid_ring(mesh):
    count = mesh.shape["fs"]
    spots = spots_of(mesh.devices.reshape(count, -1)[:, 0])
    xs = sorted({spot[0] for spot in spots})
    zs = sorted({spot[2] for spot in spots})
    if len(xs) < 2 or len(zs) % 2 or len(xs) * len(zs) != count:
        return list(range(count))
    where = {(spot[0], spot[2]): index for index, spot in enumerate(spots)}
    walk = [(xs[0], z) for z in zs]
    for turn, z in enumerate(reversed(zs)):
        inner = xs[1:] if turn % 2 == 0 else xs[:0:-1]
        walk += [(x, z) for x in inner]
    return [where[spot] for spot in walk]


def cores_of(mesh):
    spots = spots_of(mesh.devices.reshape(-1, mesh.shape["tp"])[0])
    cores = sum(spot == spots[0] for spot in spots)
    return cores if mesh.shape["tp"] % cores == 0 else 1


def tie(*values):
    return lax.optimization_barrier(values)


def dot(left, right):
    return jnp.dot(left, right, preferred_element_type=jnp.float32)


def rms_rows(rows_in, gain_vec):
    values = rows_in.astype(jnp.float32)
    scaled = (
        values * lax.rsqrt(jnp.mean(values * values, axis=-1, keepdims=True) + 1e-06) * gain_vec
    )
    return scaled.astype(jnp.bfloat16)


class Ring:
    def __init__(self, order):
        count = len(order)
        after = {order[i]: order[(i + 1) % count] for i in range(count)}
        self.count = count
        self.forward = sorted(after.items())
        self.backward = sorted((b, a) for a, b in after.items())
        owners = np.zeros((count, count), np.int32)
        for place, index in enumerate(order):
            owners[index] = [order[(place + offset) % count] for offset in range(count)]
        row = lax.dynamic_slice_in_dim(jnp.asarray(owners), lax.axis_index("fs"), 1, axis=0)[0]
        self.owners = [row[offset] for offset in range(count)]

    def owner(self, offset):
        return self.owners[offset % self.count]


class Gathered:
    def __init__(self, ring, shard, axis, block=None, start=0):
        self.ring, self.axis = ring, axis
        self.block = block or shard.shape[axis]
        self.start = start
        self.ahead = self.behind = shard
        self.size = shard.shape[axis]
        self.whole = None
        self.step = 0
        self.pieces = [(0, 0, shard)]

    def sends(self):
        self.step += 1
        last = self.ring.count - self.step
        if self.step == last:
            half = self.size // 2
            low = lax.slice_in_dim(self.ahead, 0, half, axis=self.axis)
            high = lax.slice_in_dim(self.behind, half, self.size, axis=self.axis)
            return [(low, self.ring.forward), (high, self.ring.backward)]
        return [(self.ahead, self.ring.forward), (self.behind, self.ring.backward)]

    def accept(self, ahead, behind):
        half = self.size // 2 if self.step == self.ring.count - self.step else 0
        self.ahead, self.behind = ahead, behind
        self.pieces.append((-self.step, 0, ahead))
        self.pieces.append((self.step, half, behind))

    def steps(self):
        return self.ring.count // 2


def place(items, axis):
    ring = items[0].ring
    block = items[0].block
    shape = list(items[0].pieces[0][2].shape)
    shape[axis] = block * ring.count
    whole = jnp.zeros(tuple(shape), items[0].pieces[0][2].dtype)
    for item in items:
        for offset, inside, piece in item.pieces:
            at = ring.owner(offset) * block + item.start + inside
            whole = lax.dynamic_update_slice_in_dim(whole, piece, at, axis=axis)
    return whole


class Pump:
    def __init__(self, depth):
        self.depth = depth
        self.waiting = []
        self.flying = []

    def add(self, *groups):
        steps = max(group[0].steps() for group in groups)
        for _ in range(steps):
            self.waiting += [list(group) for group in groups]

    def launch(self, value):
        group = self.waiting.pop(0)
        sends = [send for item in group for send in item.sends()]
        arrays, value = tie([array for array, _ in sends], value)
        landed = [lax.ppermute(a, "fs", way) for a, (_, way) in zip(arrays, sends)]
        self.flying.append((group, landed))
        return value

    def fill(self, value):
        while self.waiting and len(self.flying) < self.depth:
            value = self.launch(value)
        return value

    def turn(self, value, times=1):
        for _ in range(times):
            if not self.flying:
                return value
            group, landed = self.flying.pop(0)
            landed, value = tie(landed, value)
            for place_at, item in enumerate(group):
                item.accept(*landed[2 * place_at : 2 * place_at + 2])
            value = self.fill(value)
        return value


class Features:
    def __init__(self, count, cores):
        self.count, self.cores, self.chips = count, cores, count // cores
        index = lax.axis_index("tp")
        self.chip, self.core = index // cores, index % cores

    def across_core(self, value, shift):
        pairs = [
            (y * self.cores + c, y * self.cores + (c + shift) % self.cores)
            for y in range(self.chips)
            for c in range(self.cores)
        ]
        return lax.ppermute(value, "tp", pairs)

    def across_chip(self, value, shift):
        pairs = [
            (y * self.cores + c, (y + shift) % self.chips * self.cores + c)
            for y in range(self.chips)
            for c in range(self.cores)
        ]
        return lax.ppermute(value, "tp", pairs)

    def place_of(self, chip_shift, core_shift):
        chip = (self.chip - chip_shift + self.chips) % self.chips
        core = (self.core - core_shift + self.cores) % self.cores
        return chip * self.cores + core

    def gather_far(self, mine):
        return [mine] + [self.across_chip(mine, shift) for shift in range(1, self.chips)]

    def gather_near(self, far):
        size = far[0].shape[1]
        whole = jnp.zeros((far[0].shape[0], size * self.count), far[0].dtype)
        for chip_shift, piece in enumerate(far):
            for core_shift in range(self.cores):
                moved = self.across_core(piece, core_shift) if core_shift else piece
                at = self.place_of(chip_shift, core_shift) * size
                whole = lax.dynamic_update_slice_in_dim(whole, moved, at, axis=1)
        return whole

    def take(self, terms, chip, core):
        size = terms.shape[1] // self.count
        return lax.dynamic_slice_in_dim(terms, (chip * self.cores + core) * size, size, axis=1)

    def scatter_near(self, terms):
        sums = []
        for chip_shift in range(self.chips):
            chip = (self.chip + chip_shift) % self.chips
            total = self.take(terms, chip, self.core).astype(jnp.float32)
            for core_shift in range(1, self.cores):
                core = (self.core + core_shift) % self.cores
                sent = self.across_core(self.take(terms, chip, core), core_shift)
                total = total + sent.astype(jnp.float32)
            sums.append(total)
        return [sums[0]] + [total.astype(jnp.bfloat16) for total in sums[1:]]

    def scatter_far(self, sums):
        return [sums[0]] + [
            self.across_chip(total, shift) for shift, total in enumerate(sums[1:], 1)
        ]


def add_up(current, landed, factor):
    total = landed[0]
    for part in landed[1:]:
        total = total + part.astype(jnp.float32)
    return (current.astype(jnp.float32) + factor * total).astype(jnp.bfloat16)


def solution(mesh):
    order = grid_ring(mesh)
    cores = cores_of(mesh)

    def per_device(
        tokens,
        ffn_one_gain,
        ffn_one_gate,
        ffn_one_up,
        ffn_one_down,
        mix_gain,
        conv_value,
        conv_gate,
        conv_kernel,
        conv_ln_gain,
        conv_out,
        ffn_two_gain,
        ffn_two_gate,
        ffn_two_up,
        ffn_two_down,
    ):
        ring = Ring(order)
        features = Features(lax.axis_size("tp"), cores)
        channels = conv_ln_gain.shape[0] * lax.axis_size("tp")
        pump = Pump(2)

        def halves(shard, axis):
            size = shard.shape[axis]
            return [
                Gathered(
                    ring, lax.slice_in_dim(shard, low, low + size // 2, axis=axis), axis, size, low
                )
                for low in (0, size // 2)
            ]

        one_gate = Gathered(ring, ffn_one_gate, 0)
        one_up = Gathered(ring, ffn_one_up, 0)
        one_down = halves(ffn_one_down, 1)
        mix_value = Gathered(ring, conv_value, 0)
        mix_gate = Gathered(ring, conv_gate, 0)
        mix_out = Gathered(ring, conv_out, 1)
        two_gate = Gathered(ring, ffn_two_gate, 0)
        two_up = halves(ffn_two_up, 0)
        two_down = halves(ffn_two_down, 1)
        pump.add([one_gate], [one_up])
        pump.add([one_down[0]], [one_down[1]])
        pump.add([mix_value, mix_gate, mix_out], [two_gate])
        pump.add([two_up[0]], [two_up[1]])
        pump.add([two_down[0]], [two_down[1]])
        step = ring.count // 2

        tokens = pump.fill(tokens)
        far = features.gather_far(tokens)
        far = pump.turn(far, 1)
        full = features.gather_near(far)
        full = pump.turn(full, 1)
        normed = rms_rows(full, ffn_one_gain)
        normed = pump.turn(normed, 2 * step - 3)
        gate_pre = dot(normed, place([one_gate], 0))
        gate_pre = jax.nn.silu(gate_pre)
        gate_pre, normed = pump.turn((gate_pre, normed), 1)
        hidden = (gate_pre * dot(normed, place([one_up], 0))).astype(jnp.bfloat16)
        hidden = pump.turn(hidden, 2 * step)
        terms = dot(hidden, place(one_down, 1)).astype(jnp.bfloat16)
        sums = features.scatter_near(terms)
        sums = pump.turn(sums, 1)
        landed = features.scatter_far(sums)
        landed = pump.turn(landed, 1)
        stream_one = add_up(tokens, landed, 0.5)

        far = features.gather_far(stream_one)
        far = pump.turn(far, 2)
        full = features.gather_near(far)
        normed = rms_rows(full, mix_gain)
        normed = pump.turn(normed, 2 * step - 4 - 1)
        value_pre = dot(normed, place([mix_value], 0))
        gate_pre = dot(normed, place([mix_gate], 0))
        gated_lin = value_pre * jax.nn.sigmoid(gate_pre)
        half_span = conv_kernel.shape[0] // 2
        convolved = lax.conv_general_dilated(
            gated_lin[None],
            conv_kernel[:, None, :],
            (1,),
            [(half_span, half_span)],
            dimension_numbers=("NWC", "WIO", "NWC"),
            feature_group_count=gated_lin.shape[1],
            precision=lax.Precision.HIGHEST,
        )[0]
        convolved = pump.turn(convolved, 1)
        sum_one, sum_two = lax.psum(
            (jnp.sum(convolved, axis=1), jnp.sum(convolved * convolved, axis=1)), "tp"
        )
        mean_val = (sum_one / channels)[:, None]
        varied = (sum_two / channels)[:, None] - mean_val * mean_val
        active = jax.nn.silu(
            (convolved - mean_val) * lax.rsqrt(varied + 1e-05) * conv_ln_gain
        ).astype(jnp.bfloat16)
        terms = dot(active, place([mix_out], 1)).astype(jnp.bfloat16)
        sums = features.scatter_near(terms)
        sums = pump.turn(sums, 1)
        landed = features.scatter_far(sums)
        landed = pump.turn(landed, 2)
        stream_two = add_up(stream_one, landed, 1.0)

        far = features.gather_far(stream_two)
        far = pump.turn(far, 2)
        full = features.gather_near(far)
        normed = rms_rows(full, ffn_two_gain)
        gate_pre = jax.nn.silu(dot(normed, place([two_gate], 0)))
        gate_pre, normed = pump.turn((gate_pre, normed), 2 * step - 5)
        hidden = (gate_pre * dot(normed, place(two_up, 0))).astype(jnp.bfloat16)
        hidden = pump.turn(hidden, 2 * step)
        terms = dot(hidden, place(two_down, 1)).astype(jnp.bfloat16)
        landed = features.scatter_far(features.scatter_near(terms))
        return add_up(stream_two, landed, 0.5)

    in_specs = (
        P("fs", "tp"),
        P(),
        P("fs", "tp"),
        P("fs", "tp"),
        P("tp", "fs"),
        P(),
        P("fs", "tp"),
        P("fs", "tp"),
        P(None, "tp"),
        P("tp"),
        P("tp", "fs"),
        P(),
        P("fs", "tp"),
        P("fs", "tp"),
        P("tp", "fs"),
    )
    return jax.shard_map(
        per_device, mesh=mesh, in_specs=in_specs, out_specs=P("fs", "tp"), check_vma=False
    )
```

```python
import jax
import jax.numpy as jnp
import numpy as np
from jax import lax
from jax.experimental import pallas as pl
from jax.experimental.pallas import tpu as pltpu
from jax.sharding import PartitionSpec as P


def spots_of(devices):
    return [tuple(getattr(device, "coords", (0, 0, place))) for place, device in enumerate(devices)]


def grid_ring(mesh):
    count = mesh.shape["fs"]
    spots = spots_of(mesh.devices.reshape(count, -1)[:, 0])
    xs = sorted({spot[0] for spot in spots})
    zs = sorted({spot[2] for spot in spots})
    if len(xs) < 2 or len(zs) % 2 or len(xs) * len(zs) != count:
        return list(range(count))
    where = {(spot[0], spot[2]): index for index, spot in enumerate(spots)}
    walk = [(xs[0], z) for z in zs]
    for turn, z in enumerate(reversed(zs)):
        inner = xs[1:] if turn % 2 == 0 else xs[:0:-1]
        walk += [(x, z) for x in inner]
    return [where[spot] for spot in walk]


def cores_of(mesh):
    spots = spots_of(mesh.devices.reshape(-1, mesh.shape["tp"])[0])
    cores = sum(spot == spots[0] for spot in spots)
    return cores if mesh.shape["tp"] % cores == 0 else 1


def tie(*values):
    return lax.optimization_barrier(values)


def spec(space):
    return pl.BlockSpec(memory_space=space)


def hidden_kernel(blocks, rows, sides, lanes, act, spots, turn, gain, *refs):
    tokens = refs[:blocks]
    shards = [refs[blocks + i * rows : blocks + (i + 1) * rows] for i in range(sides)]
    out, normed, left, right, sems = refs[blocks + sides * rows :]
    depth = shards[0][0].shape[0]
    width = left.shape[1]
    copies = []
    for which, whole in enumerate((left, right)):
        source = shards[which % sides]
        for slot in range(rows):
            at = pl.multiple_of(spots[slot] * depth, depth)
            copies.append(
                pltpu.make_async_copy(
                    source[slot].at[:, pl.ds(lanes[which], width)],
                    whole.at[pl.ds(at, depth), :],
                    sems.at[which, slot],
                )
            )
    for copy in copies:
        copy.start()

    count, size = tokens[0].shape
    step = 64 if count % 64 == 0 else count

    @pl.loop(0, count // step)
    def _(index):
        here = pl.ds(pl.multiple_of(index * step, step), step)
        parts = [token[here, :].astype(jnp.float32) for token in tokens]
        total = sum(jnp.sum(part * part, axis=1, keepdims=True) for part in parts)
        scale = lax.rsqrt(total / (size * blocks) + 1e-06)
        for place_at, part in enumerate(parts):
            scaled = part * scale * gain[turn[place_at]]
            normed[here, place_at * size : (place_at + 1) * size] = scaled.astype(jnp.bfloat16)

    for copy in copies:
        copy.wait()

    def product(whole, here):
        return jnp.dot(normed[...], whole[:, here], preferred_element_type=jnp.float32)

    tile = 256
    whole_tiles = width // tile

    @pl.loop(0, whole_tiles)
    def _(index):
        here = pl.ds(pl.multiple_of(index * tile, tile), tile)
        out[:, here] = act(product(left, here), product(right, here)).astype(out.dtype)

    rest = width - whole_tiles * tile
    if rest:
        here = pl.ds(whole_tiles * tile, rest)
        if rest % 128 == 0:
            both = jnp.concatenate([left[:, here], right[:, here]], axis=1)
            pair = jnp.dot(normed[...], both, preferred_element_type=jnp.float32)
            out[:, here] = act(pair[:, :rest], pair[:, rest:]).astype(out.dtype)
        else:
            out[:, here] = act(product(left, here), product(right, here)).astype(out.dtype)


def terms_kernel(slots, parts, low, cores, whose, where, inside, hidden, *refs):
    shards = refs[: slots * parts]
    outs = refs[slots * parts : slots * parts + cores]
    columns, sems = refs[slots * parts + cores :]
    width = columns.shape[2]
    copies = [
        pltpu.make_async_copy(
            shards[part * slots + slot].at[:, pl.ds(low, width)],
            columns.at[slot, pl.ds(part * shards[0].shape[0], shards[0].shape[0]), :],
            sems.at[part, slot],
        )
        for slot in range(slots)
        for part in range(parts)
    ]
    for copy in copies:
        copy.start()
    for copy in copies:
        copy.wait()

    @pl.loop(0, slots)
    def _(slot):
        value = jnp.dot(hidden[...], columns[slot], preferred_element_type=jnp.float32)
        value = value.astype(jnp.bfloat16)
        here = pl.ds(pl.multiple_of(inside[slot] * width, width), width)
        for core in range(cores):

            @pl.when(whose[slot] == core)
            def _(core=core):
                outs[core][where[slot], :, here] = value


def silu_times(gate, up):
    return gate / (1.0 + jnp.exp(-gate)) * up


def gate_times(gate, value):
    return value / (1.0 + jnp.exp(-gate))


class Ring:
    def __init__(self, order):
        count = len(order)
        after = {order[i]: order[(i + 1) % count] for i in range(count)}
        self.count = count
        self.forward = sorted(after.items())
        self.backward = sorted((b, a) for a, b in after.items())
        owners = np.zeros((count, count), np.int32)
        for place, index in enumerate(order):
            owners[index] = [order[(place + offset) % count] for offset in range(count)]
        row = lax.dynamic_slice_in_dim(jnp.asarray(owners), lax.axis_index("fs"), 1, axis=0)
        self.owners = row[0]


class Gathered:
    def __init__(self, ring, shard, onward):
        self.ring, self.onward = ring, onward
        self.ahead = self.behind = shard
        self.step = 0
        self.shards = {0: shard}

    def steps(self):
        return self.ring.count // 2

    def complete(self):
        return len(self.shards) == self.ring.count

    def ways(self):
        if self.step < self.ring.count - self.step:
            return (True, False)
        return (self.onward,)

    def sends(self):
        self.step += 1
        return [
            (self.ahead, self.ring.forward) if onward else (self.behind, self.ring.backward)
            for onward in self.ways()
        ]

    def accept(self, landed):
        for onward in self.ways():
            shard = landed.pop(0)
            if onward:
                self.ahead = shard
                self.shards[self.ring.count - self.step] = shard
            else:
                self.behind = shard
                self.shards[self.step] = shard

    def listed(self):
        return [self.shards[offset] for offset in range(self.ring.count)]


class Pump:
    def __init__(self, depth):
        self.depth = depth
        self.waiting = []
        self.flying = []
        self.sent = 0
        self.mark = lax.axis_index("fs")

    def add(self, *groups):
        steps = max(group[0].steps() for group in groups)
        for _ in range(steps):
            self.waiting += [list(group) for group in groups]

    def launch(self, value):
        group = self.waiting.pop(0)
        sends = [send for item in group for send in item.sends()]
        arrays, value = tie([array for array, _ in sends], value)
        landed = [lax.ppermute(a, "fs", way) for a, (_, way) in zip(arrays, sends)]
        self.flying.append((group, landed, self.sent))
        self.sent += 1
        return value

    def fill(self, value):
        while self.waiting and len(self.flying) < self.depth:
            value = self.launch(value)
        return value

    def until(self, items, value):
        while not all(item.complete() for item in items):
            value = self.turn(value)
        return value

    def turn(self, value, times=1):
        for _ in range(times):
            if not self.flying:
                return value
            group, landed, _ = self.flying.pop(0)
            landed, self.mark, value = tie(landed, self.mark, value)
            landed = list(landed)
            for item in group:
                item.accept(landed)
            self.mark, value = self.fill((self.mark, value))
            if len(self.flying) == self.depth:
                self.mark = self.mark + 1
                self.mark, value = tie(self.mark, value)
        return value


class Features:
    def __init__(self, count, cores):
        self.count, self.cores, self.chips = count, cores, count // cores
        index = lax.axis_index("tp")
        self.chip, self.core = index // cores, index % cores

    def across_core(self, value, shift):
        pairs = [
            (y * self.cores + c, y * self.cores + (c + shift) % self.cores)
            for y in range(self.chips)
            for c in range(self.cores)
        ]
        return lax.ppermute(value, "tp", pairs)

    def across_chip(self, value, shift):
        pairs = [
            (y * self.cores + c, (y + shift) % self.chips * self.cores + c)
            for y in range(self.chips)
            for c in range(self.cores)
        ]
        return lax.ppermute(value, "tp", pairs)

    def place_of(self, chip_shift, core_shift):
        chip = (self.chip - chip_shift + self.chips) % self.chips
        core = (self.core - core_shift + self.cores) % self.cores
        return chip * self.cores + core

    def gather_far(self, mine):
        return [mine] + [self.across_chip(mine, shift) for shift in range(1, self.chips)]

    def gather_near(self, far):
        return [
            self.across_core(piece, shift) if shift else piece
            for piece in far
            for shift in range(self.cores)
        ]

    def blocks(self):
        return jnp.stack(
            [
                (self.chip - chip + self.chips) % self.chips * self.cores
                + (self.core - core + self.cores) % self.cores
                for chip in range(self.chips)
                for core in range(self.cores)
            ]
        )

    def spots(self, owners, each):
        holder = owners // each
        chip = (self.chip - holder // self.cores + self.chips) % self.chips
        core = (self.core - holder % self.cores + self.cores) % self.cores
        return (chip * self.cores + core) * each + owners % each

    def targets(self, owners, each):
        holder = owners // each
        chip = (holder // self.cores - self.chip + self.chips) % self.chips
        core = (holder % self.cores - self.core + self.cores) % self.cores
        return core, chip, owners % each

    def scatter_near(self, terms):
        sent = [self.across_core(part, shift) for shift, part in enumerate(terms[1:], 1)]
        total = terms[0].astype(jnp.float32)
        for part in sent:
            total = total + part.astype(jnp.float32)
        return [total[0]] + [total[chip].astype(jnp.bfloat16) for chip in range(1, self.chips)]

    def scatter_far(self, sums):
        return [sums[0]] + [
            self.across_chip(total, shift) for shift, total in enumerate(sums[1:], 1)
        ]


def add_up(current, landed, factor):
    total = landed[0]
    for part in landed[1:]:
        total = total + part.astype(jnp.float32)
    return (current.astype(jnp.float32) + factor * total).astype(jnp.bfloat16)


def solution(mesh):
    order = grid_ring(mesh)
    cores = cores_of(mesh)
    depth = 2

    def per_device(
        tokens,
        ffn_one_gain,
        ffn_one_gate,
        ffn_one_up,
        ffn_one_down,
        mix_gain,
        conv_value,
        conv_gate,
        conv_kernel,
        conv_ln_gain,
        conv_out,
        ffn_two_gain,
        ffn_two_gate,
        ffn_two_up,
        ffn_two_down,
    ):
        ring = Ring(order)
        features = Features(lax.axis_size("tp"), cores)
        channels = conv_ln_gain.shape[0] * lax.axis_size("tp")
        pump = Pump(depth)
        wide = conv_value.shape[1]
        half = ffn_two_down.shape[0] // 2
        one_gate = Gathered(ring, ffn_one_gate, True)
        one_up = Gathered(ring, ffn_one_up, False)
        one_down = Gathered(ring, ffn_one_down, True)
        if conv_value.shape[0] == conv_out.shape[0]:
            mixed = jnp.concatenate([conv_value, conv_gate, conv_out], axis=1)
            mix_in = mix_out = Gathered(ring, mixed, False)
            mixes, out_from = [mix_in], 2 * wide
        else:
            mix_in = Gathered(ring, jnp.concatenate([conv_value, conv_gate], axis=1), False)
            mix_out, out_from = Gathered(ring, conv_out, False), 0
            mixes = [mix_in, mix_out]
        two_gate = Gathered(ring, ffn_two_gate, True)
        two_up = Gathered(ring, ffn_two_up, False)
        two_down = [
            Gathered(ring, ffn_two_down[:half], True),
            Gathered(ring, ffn_two_down[half:], False),
        ]
        pump.add([one_gate], [one_up])
        pump.add([one_down], mixes)
        pump.add([two_gate], [two_up])
        pump.add([two_down[0]], [two_down[1]])

        count = features.count
        each = ring.count // count
        blocks = features.blocks()
        spots = features.spots(ring.owners, each)
        targets = features.targets(ring.owners, each)
        vmem, smem, hbm = pltpu.VMEM, pltpu.SMEM, pltpu.HBM

        def hidden_of(parts, gain_vec, sides, lanes, width, act, dtype):
            length, size = parts[0].shape
            rows = count * size
            arrays = [shard for side in sides for shard in side.listed()]
            return pl.pallas_call(
                lambda *refs: hidden_kernel(
                    count, ring.count, len(sides), lanes, act, *refs
                ),
                out_shape=jax.ShapeDtypeStruct((length, width), dtype),
                in_specs=[spec(smem)] * 2 + [spec(vmem)] * (1 + count) + [spec(hbm)] * len(arrays),
                out_specs=spec(vmem),
                scratch_shapes=[
                    pltpu.VMEM((length, rows), jnp.bfloat16),
                    pltpu.VMEM((rows, width), jnp.bfloat16),
                    pltpu.VMEM((rows, width), jnp.bfloat16),
                    pltpu.SemaphoreType.DMA((2, ring.count)),
                ],
                cost_estimate=pl.CostEstimate(
                    flops=4 * length * rows * width,
                    bytes_accessed=4 * rows * width + 2 * length * rows,
                    transcendentals=length * width,
                ),
                name="hidden",
            )(spots, blocks, gain_vec.reshape(count, 1, size), *parts, *arrays)

        def terms_of(hidden, sides, low, width):
            length, depth_all = hidden.shape
            arrays = [shard for side in sides for shard in side.listed()]
            out = jax.ShapeDtypeStruct((features.chips, length, each * width), jnp.bfloat16)
            return pl.pallas_call(
                lambda *refs: terms_kernel(ring.count, len(sides), low, cores, *refs),
                out_shape=[out] * cores,
                in_specs=[spec(smem)] * 3 + [spec(vmem)] + [spec(hbm)] * len(arrays),
                out_specs=[spec(vmem)] * cores,
                scratch_shapes=[
                    pltpu.VMEM((ring.count, depth_all, width), jnp.bfloat16),
                    pltpu.SemaphoreType.DMA((len(sides), ring.count)),
                ],
                cost_estimate=pl.CostEstimate(
                    flops=2 * length * depth_all * ring.count * width,
                    bytes_accessed=2 * depth_all * ring.count * width,
                    transcendentals=0,
                ),
                name="terms",
            )(*targets, hidden, *arrays)

        tokens = pump.fill(tokens)
        far = features.gather_far(tokens)
        far = pump.turn(far)
        parts = features.gather_near(far)
        parts = pump.until([one_gate, one_up], parts)
        hidden = hidden_of(
            parts, ffn_one_gain, [one_gate, one_up], (0, 0), ffn_one_up.shape[1], silu_times,
            jnp.bfloat16,
        )
        hidden = pump.until([one_down], hidden)
        terms = terms_of(hidden, [one_down], 0, ffn_one_down.shape[1])
        sums = pump.turn(features.scatter_near(terms))
        landed = features.scatter_far(sums)
        pump.turn(())
        stream_one = add_up(tokens, landed, 0.5)

        stream_one = pump.until(mixes, stream_one)
        far = features.gather_far(stream_one)
        pump.turn((), 2)
        parts = pump.turn(features.gather_near(far))
        gated_lin = hidden_of(
            parts, mix_gain, [mix_in], (wide, 0), wide, gate_times, jnp.float32
        )
        half_span = conv_kernel.shape[0] // 2
        convolved = lax.conv_general_dilated(
            gated_lin[None],
            conv_kernel[:, None, :],
            (1,),
            [(half_span, half_span)],
            dimension_numbers=("NWC", "WIO", "NWC"),
            feature_group_count=gated_lin.shape[1],
            precision=lax.Precision.HIGHEST,
        )[0]
        convolved = pump.turn(convolved)
        sum_one, sum_two = lax.psum(
            (jnp.sum(convolved, axis=1), jnp.sum(convolved * convolved, axis=1)), "tp"
        )
        mean_val = (sum_one / channels)[:, None]
        varied = (sum_two / channels)[:, None] - mean_val * mean_val
        active = jax.nn.silu(
            (convolved - mean_val) * lax.rsqrt(varied + 1e-05) * conv_ln_gain
        ).astype(jnp.bfloat16)
        terms = terms_of(active, [mix_out], out_from, conv_out.shape[1])
        sums = pump.turn(features.scatter_near(terms))
        landed = features.scatter_far(sums)
        pump.turn(())
        stream_two = pump.turn(add_up(stream_one, landed, 1.0))

        far = features.gather_far(stream_two)
        pump.turn((), 2)
        parts = features.gather_near(far)
        parts = pump.until([two_gate, two_up], parts)
        hidden = hidden_of(
            parts, ffn_two_gain, [two_gate, two_up], (0, 0), ffn_two_up.shape[1], silu_times,
            jnp.bfloat16,
        )
        hidden = pump.until(two_down, hidden)
        terms = terms_of(hidden, two_down, 0, ffn_two_down.shape[1])
        landed = features.scatter_far(features.scatter_near(terms))
        return jnp.where(pump.mark < 0, stream_two, add_up(stream_two, landed, 0.5))

    in_specs = (
        P("fs", "tp"),
        P(),
        P("fs", "tp"),
        P("fs", "tp"),
        P("tp", "fs"),
        P(),
        P("fs", "tp"),
        P("fs", "tp"),
        P(None, "tp"),
        P("tp"),
        P("tp", "fs"),
        P(),
        P("fs", "tp"),
        P("fs", "tp"),
        P("tp", "fs"),
    )
    return jax.shard_map(
        per_device, mesh=mesh, in_specs=in_specs, out_specs=P("fs", "tp"), check_vma=False
    )
```

```python
import jax
import jax.numpy as jnp
import numpy as np
from jax import lax
from jax.experimental import pallas as pl
from jax.experimental.pallas import tpu as pltpu
from jax.sharding import PartitionSpec as P


def spots_of(devices):
    return [tuple(getattr(device, "coords", (0, 0, place))) for place, device in enumerate(devices)]


def grid_ring(mesh):
    count = mesh.shape["fs"]
    spots = spots_of(mesh.devices.reshape(count, -1)[:, 0])
    xs = sorted({spot[0] for spot in spots})
    zs = sorted({spot[2] for spot in spots})
    if len(xs) < 2 or len(zs) % 2 or len(xs) * len(zs) != count:
        return list(range(count))
    where = {(spot[0], spot[2]): index for index, spot in enumerate(spots)}
    walk = [(xs[0], z) for z in zs]
    for turn, z in enumerate(reversed(zs)):
        inner = xs[1:] if turn % 2 == 0 else xs[:0:-1]
        walk += [(x, z) for x in inner]
    return [where[spot] for spot in walk]


def cores_of(mesh):
    spots = spots_of(mesh.devices.reshape(-1, mesh.shape["tp"])[0])
    cores = sum(spot == spots[0] for spot in spots)
    return cores if mesh.shape["tp"] % cores == 0 else 1


def tie(*values):
    return lax.optimization_barrier(values)


def spec(space):
    return pl.BlockSpec(memory_space=space)


def hidden_kernel(blocks, rows, sides, lanes, act, spots, turn, gain, *refs):
    tokens = refs[:blocks]
    shards = [refs[blocks + i * rows : blocks + (i + 1) * rows] for i in range(sides)]
    out, normed, left, right, sems = refs[blocks + sides * rows :]
    depth = shards[0][0].shape[0]
    width = left.shape[1]
    copies = []
    for which, whole in enumerate((left, right)):
        source = shards[which % sides]
        for slot in range(rows):
            at = pl.multiple_of(spots[slot] * depth, depth)
            copies.append(
                pltpu.make_async_copy(
                    source[slot].at[:, pl.ds(lanes[which], width)],
                    whole.at[pl.ds(at, depth), :],
                    sems.at[which, slot],
                )
            )
    for copy in copies:
        copy.start()

    count, size = tokens[0].shape
    step = 64 if count % 64 == 0 else count

    @pl.loop(0, count // step)
    def _(index):
        here = pl.ds(pl.multiple_of(index * step, step), step)
        parts = [token[here, :].astype(jnp.float32) for token in tokens]
        total = sum(jnp.sum(part * part, axis=1, keepdims=True) for part in parts)
        scale = lax.rsqrt(total / (size * blocks) + 1e-06)
        for place_at, part in enumerate(parts):
            scaled = part * scale * gain[turn[place_at]]
            normed[here, place_at * size : (place_at + 1) * size] = scaled.astype(jnp.bfloat16)

    for copy in copies:
        copy.wait()

    def product(whole, here):
        return jnp.dot(normed[...], whole[:, here], preferred_element_type=jnp.float32)

    tile = 256
    whole_tiles = width // tile

    @pl.loop(0, whole_tiles)
    def _(index):
        here = pl.ds(pl.multiple_of(index * tile, tile), tile)
        out[:, here] = act(product(left, here), product(right, here)).astype(out.dtype)

    rest = width - whole_tiles * tile
    if rest:
        here = pl.ds(whole_tiles * tile, rest)
        if rest % 128 == 0:
            both = jnp.concatenate([left[:, here], right[:, here]], axis=1)
            pair = jnp.dot(normed[...], both, preferred_element_type=jnp.float32)
            out[:, here] = act(pair[:, :rest], pair[:, rest:]).astype(out.dtype)
        else:
            out[:, here] = act(product(left, here), product(right, here)).astype(out.dtype)


def terms_kernel(slots, parts, low, cores, far, whose, where, inside, hidden, *refs):
    shards = refs[: slots * parts]
    outs = refs[slots * parts : slots * parts + cores]
    columns, sems = refs[slots * parts + cores :]
    depth, width = shards[0].shape[0], columns.shape[2]

    def wanted(slot):
        return where[slot] > 0 if far else where[slot] == 0

    for slot in range(slots):

        @pl.when(wanted(slot))
        def _(slot=slot):
            for part in range(parts):
                pltpu.make_async_copy(
                    shards[part * slots + slot].at[:, pl.ds(low, width)],
                    columns.at[slot, pl.ds(part * depth, depth), :],
                    sems.at[part, slot],
                ).start()

    @pl.loop(0, slots)
    def _(slot):
        @pl.when(wanted(slot))
        def _():
            for part in range(parts):
                landing = columns.at[slot, pl.ds(part * depth, depth), :]
                pltpu.make_async_copy(landing, landing, sems.at[part, slot]).wait()
            value = jnp.dot(hidden[...], columns[slot], preferred_element_type=jnp.float32)
            value = value.astype(jnp.bfloat16)
            here = pl.ds(pl.multiple_of(inside[slot] * width, width), width)
            to = where[slot] - 1 if far else 0
            for core in range(cores):

                @pl.when(whose[slot] == core)
                def _(core=core):
                    outs[core][to, :, here] = value


def silu_times(gate, up):
    return gate / (1.0 + jnp.exp(-gate)) * up


def gate_times(gate, value):
    return value / (1.0 + jnp.exp(-gate))


class Ring:
    def __init__(self, order):
        count = len(order)
        after = {order[i]: order[(i + 1) % count] for i in range(count)}
        self.count = count
        self.forward = sorted(after.items())
        self.backward = sorted((b, a) for a, b in after.items())
        owners = np.zeros((count, count), np.int32)
        for place, index in enumerate(order):
            owners[index] = [order[(place + offset) % count] for offset in range(count)]
        row = lax.dynamic_slice_in_dim(jnp.asarray(owners), lax.axis_index("fs"), 1, axis=0)
        self.owners = row[0]


class Gathered:
    def __init__(self, ring, shard, onward):
        self.ring, self.onward = ring, onward
        self.ahead = self.behind = shard
        self.step = 0
        self.shards = {0: shard}

    def steps(self):
        return self.ring.count // 2

    def complete(self):
        return len(self.shards) == self.ring.count

    def ways(self):
        if self.step < self.ring.count - self.step:
            return (True, False)
        return (self.onward,)

    def sends(self):
        self.step += 1
        return [
            (self.ahead, self.ring.forward) if onward else (self.behind, self.ring.backward)
            for onward in self.ways()
        ]

    def accept(self, landed):
        for onward in self.ways():
            shard = landed.pop(0)
            if onward:
                self.ahead = shard
                self.shards[self.ring.count - self.step] = shard
            else:
                self.behind = shard
                self.shards[self.step] = shard

    def listed(self):
        return [self.shards[offset] for offset in range(self.ring.count)]


class Pump:
    def __init__(self, depth):
        self.depth = depth
        self.waiting = []
        self.flying = []
        self.sent = 0
        self.mark = lax.axis_index("fs")

    def add(self, *groups):
        steps = max(group[0].steps() for group in groups)
        for _ in range(steps):
            self.waiting += [list(group) for group in groups]

    def launch(self, value):
        group = self.waiting.pop(0)
        sends = [send for item in group for send in item.sends()]
        arrays, value = tie([array for array, _ in sends], value)
        landed = [lax.ppermute(a, "fs", way) for a, (_, way) in zip(arrays, sends)]
        self.flying.append((group, landed, self.sent))
        self.sent += 1
        return value

    def fill(self, value):
        while self.waiting and len(self.flying) < self.depth:
            value = self.launch(value)
        return value

    def until(self, items, value):
        while not all(item.complete() for item in items):
            value = self.turn(value)
        return value

    def turn(self, value, times=1):
        for _ in range(times):
            if not self.flying:
                return value
            group, landed, _ = self.flying.pop(0)
            landed, self.mark, value = tie(landed, self.mark, value)
            landed = list(landed)
            for item in group:
                item.accept(landed)
            self.mark, value = self.fill((self.mark, value))
            if len(self.flying) == self.depth:
                self.mark = self.mark + 1
                self.mark, value = tie(self.mark, value)
        return value


class Features:
    def __init__(self, count, cores):
        self.count, self.cores, self.chips = count, cores, count // cores
        index = lax.axis_index("tp")
        self.chip, self.core = index // cores, index % cores

    def across_core(self, value, shift):
        pairs = [
            (y * self.cores + c, y * self.cores + (c + shift) % self.cores)
            for y in range(self.chips)
            for c in range(self.cores)
        ]
        return lax.ppermute(value, "tp", pairs)

    def across_chip(self, value, shift):
        pairs = [
            (y * self.cores + c, (y + shift) % self.chips * self.cores + c)
            for y in range(self.chips)
            for c in range(self.cores)
        ]
        return lax.ppermute(value, "tp", pairs)

    def place_of(self, chip_shift, core_shift):
        chip = (self.chip - chip_shift + self.chips) % self.chips
        core = (self.core - core_shift + self.cores) % self.cores
        return chip * self.cores + core

    def gather_far(self, mine):
        return [self.across_chip(mine, shift) for shift in range(1, self.chips)]

    def gather_near(self, far):
        return [
            self.across_core(piece, shift) if shift else piece
            for piece in far
            for shift in range(self.cores)
        ]

    def blocks(self):
        return jnp.stack(
            [
                (self.chip - chip + self.chips) % self.chips * self.cores
                + (self.core - core + self.cores) % self.cores
                for chip in range(self.chips)
                for core in range(self.cores)
            ]
        )

    def spots(self, owners, each):
        holder = owners // each
        chip = (self.chip - holder // self.cores + self.chips) % self.chips
        core = (self.core - holder % self.cores + self.cores) % self.cores
        return (chip * self.cores + core) * each + owners % each

    def targets(self, owners, each):
        holder = owners // each
        chip = (holder // self.cores - self.chip + self.chips) % self.chips
        core = (holder % self.cores - self.core + self.cores) % self.cores
        return core, chip, owners % each

    def over_cores(self, terms):
        sent = [self.across_core(part, shift) for shift, part in enumerate(terms[1:], 1)]
        total = terms[0].astype(jnp.float32)
        for part in sent:
            total = total + part.astype(jnp.float32)
        return total

    def over_chips(self, sums):
        sums = sums.astype(jnp.bfloat16)
        return [self.across_chip(sums[shift - 1], shift) for shift in range(1, self.chips)]


def add_up(current, own, landed, factor):
    total = own[0]
    for part in landed:
        total = total + part.astype(jnp.float32)
    return (current.astype(jnp.float32) + factor * total).astype(jnp.bfloat16)


def solution(mesh):
    order = grid_ring(mesh)
    cores = cores_of(mesh)
    depth = 2

    def per_device(
        tokens,
        ffn_one_gain,
        ffn_one_gate,
        ffn_one_up,
        ffn_one_down,
        mix_gain,
        conv_value,
        conv_gate,
        conv_kernel,
        conv_ln_gain,
        conv_out,
        ffn_two_gain,
        ffn_two_gate,
        ffn_two_up,
        ffn_two_down,
    ):
        ring = Ring(order)
        features = Features(lax.axis_size("tp"), cores)
        channels = conv_ln_gain.shape[0] * lax.axis_size("tp")
        pump = Pump(depth)
        wide = conv_value.shape[1]
        half = ffn_two_down.shape[0] // 2
        one_gate = Gathered(ring, ffn_one_gate, True)
        one_up = Gathered(ring, ffn_one_up, False)
        one_down = Gathered(ring, ffn_one_down, True)
        if conv_value.shape[0] == conv_out.shape[0]:
            mixed = jnp.concatenate([conv_value, conv_gate, conv_out], axis=1)
            mix_in = mix_out = Gathered(ring, mixed, False)
            mixes, out_from = [mix_in], 2 * wide
        else:
            mix_in = Gathered(ring, jnp.concatenate([conv_value, conv_gate], axis=1), False)
            mix_out, out_from = Gathered(ring, conv_out, False), 0
            mixes = [mix_in, mix_out]
        two_gate = Gathered(ring, ffn_two_gate, True)
        two_up = Gathered(ring, ffn_two_up, False)
        two_down = [
            Gathered(ring, ffn_two_down[:half], True),
            Gathered(ring, ffn_two_down[half:], False),
        ]
        pump.add([one_gate], [one_up])
        pump.add([one_down], mixes)
        pump.add([two_gate], [two_up])
        pump.add([two_down[0]], [two_down[1]])

        count = features.count
        each = ring.count // count
        blocks = features.blocks()
        spots = features.spots(ring.owners, each)
        targets = features.targets(ring.owners, each)
        vmem, smem, hbm = pltpu.VMEM, pltpu.SMEM, pltpu.HBM

        def hidden_of(parts, gain_vec, sides, lanes, width, act, dtype):
            length, size = parts[0].shape
            rows = count * size
            arrays = [shard for side in sides for shard in side.listed()]
            return pl.pallas_call(
                lambda *refs: hidden_kernel(
                    count, ring.count, len(sides), lanes, act, *refs
                ),
                out_shape=jax.ShapeDtypeStruct((length, width), dtype),
                in_specs=[spec(smem)] * 2 + [spec(vmem)] * (1 + count) + [spec(hbm)] * len(arrays),
                out_specs=spec(vmem),
                scratch_shapes=[
                    pltpu.VMEM((length, rows), jnp.bfloat16),
                    pltpu.VMEM((rows, width), jnp.bfloat16),
                    pltpu.VMEM((rows, width), jnp.bfloat16),
                    pltpu.SemaphoreType.DMA((2, ring.count)),
                ],
                cost_estimate=pl.CostEstimate(
                    flops=4 * length * rows * width,
                    bytes_accessed=4 * rows * width + 2 * length * rows,
                    transcendentals=length * width,
                ),
                name="hidden",
            )(spots, blocks, gain_vec.reshape(count, 1, size), *parts, *arrays)

        def terms_of(hidden, sides, low, width, far):
            length, depth_all = hidden.shape
            arrays = [shard for side in sides for shard in side.listed()]
            chips = features.chips - 1 if far else 1
            out = jax.ShapeDtypeStruct((chips, length, each * width), jnp.bfloat16)
            return pl.pallas_call(
                lambda *refs: terms_kernel(ring.count, len(sides), low, cores, far, *refs),
                out_shape=[out] * cores,
                in_specs=[spec(smem)] * 3 + [spec(vmem)] + [spec(hbm)] * len(arrays),
                out_specs=[spec(vmem)] * cores,
                scratch_shapes=[
                    pltpu.VMEM((ring.count, depth_all, width), jnp.bfloat16),
                    pltpu.SemaphoreType.DMA((len(sides), ring.count)),
                ],
                cost_estimate=pl.CostEstimate(
                    flops=2 * length * depth_all * chips * cores * each * width,
                    bytes_accessed=2 * depth_all * chips * cores * each * width,
                    transcendentals=0,
                ),
                name="far_terms" if far else "near_terms",
            )(*targets, hidden, *arrays)

        def scatter(hidden, sides, low, width, turns):
            landed = []
            if features.chips > 1:
                sums = features.over_cores(terms_of(hidden, sides, low, width, True))
                hidden, sums = tie(hidden, sums)
                landed = features.over_chips(sums)
            terms = terms_of(hidden, sides, low, width, False)
            own = features.over_cores(terms)
            return pump.turn(own, turns), landed

        tokens = pump.fill(tokens)
        far = features.gather_far(tokens)
        far = pump.turn(far)
        parts = features.gather_near([tokens] + far)
        parts = pump.until([one_gate, one_up], parts)
        hidden = hidden_of(
            parts, ffn_one_gain, [one_gate, one_up], (0, 0), ffn_one_up.shape[1], silu_times,
            jnp.bfloat16,
        )
        hidden = pump.until([one_down] + mixes, hidden)
        own, landed = scatter(hidden, [one_down], 0, ffn_one_down.shape[1], 1)
        stream_one = add_up(tokens, own, landed, 0.5)

        far = features.gather_far(stream_one)
        stream_one = pump.turn(stream_one, 2)
        parts = features.gather_near([stream_one] + far)
        gated_lin = hidden_of(
            parts, mix_gain, [mix_in], (wide, 0), wide, gate_times, jnp.float32
        )
        half_span = conv_kernel.shape[0] // 2
        convolved = lax.conv_general_dilated(
            gated_lin[None],
            conv_kernel[:, None, :],
            (1,),
            [(half_span, half_span)],
            dimension_numbers=("NWC", "WIO", "NWC"),
            feature_group_count=gated_lin.shape[1],
            precision=lax.Precision.HIGHEST,
        )[0]
        convolved = pump.turn(convolved)
        sum_one, sum_two = lax.psum(
            (jnp.sum(convolved, axis=1), jnp.sum(convolved * convolved, axis=1)), "tp"
        )
        mean_val = (sum_one / channels)[:, None]
        varied = (sum_two / channels)[:, None] - mean_val * mean_val
        active = jax.nn.silu(
            (convolved - mean_val) * lax.rsqrt(varied + 1e-05) * conv_ln_gain
        ).astype(jnp.bfloat16)
        active = pump.turn(active)
        own, landed = scatter(active, [mix_out], out_from, conv_out.shape[1], 1)
        stream_two = add_up(stream_one, own, landed, 1.0)

        far = features.gather_far(stream_two)
        stream_two = pump.turn(stream_two, 3)
        parts = features.gather_near([stream_two] + far)
        parts = pump.until([two_gate, two_up], pump.turn(parts))
        hidden = hidden_of(
            parts, ffn_two_gain, [two_gate, two_up], (0, 0), ffn_two_up.shape[1], silu_times,
            jnp.bfloat16,
        )
        hidden = pump.until(two_down, hidden)
        own, landed = scatter(hidden, two_down, 0, ffn_two_down.shape[1], 0)
        return jnp.where(pump.mark < 0, stream_two, add_up(stream_two, own, landed, 0.5))

    in_specs = (
        P("fs", "tp"),
        P(),
        P("fs", "tp"),
        P("fs", "tp"),
        P("tp", "fs"),
        P(),
        P("fs", "tp"),
        P("fs", "tp"),
        P(None, "tp"),
        P("tp"),
        P("tp", "fs"),
        P(),
        P("fs", "tp"),
        P("fs", "tp"),
        P("tp", "fs"),
    )
    return jax.shard_map(
        per_device, mesh=mesh, in_specs=in_specs, out_specs=P("fs", "tp"), check_vma=False
    )
```

```python
import jax
import jax.numpy as jnp
import numpy as np
from jax import lax
from jax.experimental import pallas as pl
from jax.experimental.pallas import tpu as pltpu
from jax.sharding import PartitionSpec as P


def spots_of(devices):
    return [tuple(getattr(device, "coords", (0, 0, place))) for place, device in enumerate(devices)]


def grid_ring(mesh):
    count = mesh.shape["fs"]
    spots = spots_of(mesh.devices.reshape(count, -1)[:, 0])
    xs = sorted({spot[0] for spot in spots})
    zs = sorted({spot[2] for spot in spots})
    if len(xs) < 2 or len(zs) % 2 or len(xs) * len(zs) != count:
        return list(range(count))
    where = {(spot[0], spot[2]): index for index, spot in enumerate(spots)}
    walk = [(xs[0], z) for z in zs]
    for turn, z in enumerate(reversed(zs)):
        inner = xs[1:] if turn % 2 == 0 else xs[:0:-1]
        walk += [(x, z) for x in inner]
    return [where[spot] for spot in walk]


def cores_of(mesh):
    spots = spots_of(mesh.devices.reshape(-1, mesh.shape["tp"])[0])
    cores = sum(spot == spots[0] for spot in spots)
    return cores if mesh.shape["tp"] % cores == 0 else 1


def tie(*values):
    return lax.optimization_barrier(values)


def spec(space):
    return pl.BlockSpec(memory_space=space)


def hidden_kernel(blocks, rows, sides, lanes, act, spots, turn, gain, *refs):
    tokens = refs[:blocks]
    shards = [refs[blocks + i * rows : blocks + (i + 1) * rows] for i in range(sides)]
    out, normed, left, right, sems = refs[blocks + sides * rows :]
    depth = shards[0][0].shape[0]
    width = left.shape[1]
    copies = []
    for which, whole in enumerate((left, right)):
        source = shards[which % sides]
        for slot in range(rows):
            at = pl.multiple_of(spots[slot] * depth, depth)
            copies.append(
                pltpu.make_async_copy(
                    source[slot].at[:, pl.ds(lanes[which], width)],
                    whole.at[pl.ds(at, depth), :],
                    sems.at[which, slot],
                )
            )
    for copy in copies:
        copy.start()

    count, size = tokens[0].shape
    step = 64 if count % 64 == 0 else count

    @pl.loop(0, count // step)
    def _(index):
        here = pl.ds(pl.multiple_of(index * step, step), step)
        parts = [token[here, :].astype(jnp.float32) for token in tokens]
        total = sum(jnp.sum(part * part, axis=1, keepdims=True) for part in parts)
        scale = lax.rsqrt(total / (size * blocks) + 1e-06)
        for place_at, part in enumerate(parts):
            scaled = part * scale * gain[turn[place_at]]
            normed[here, place_at * size : (place_at + 1) * size] = scaled.astype(jnp.bfloat16)

    for copy in copies:
        copy.wait()

    def product(whole, here):
        return jnp.dot(normed[...], whole[:, here], preferred_element_type=jnp.float32)

    tile = 256
    whole_tiles = width // tile

    @pl.loop(0, whole_tiles)
    def _(index):
        here = pl.ds(pl.multiple_of(index * tile, tile), tile)
        out[:, here] = act(product(left, here), product(right, here)).astype(out.dtype)

    rest = width - whole_tiles * tile
    if rest:
        here = pl.ds(whole_tiles * tile, rest)
        if rest % 128 == 0:
            both = jnp.concatenate([left[:, here], right[:, here]], axis=1)
            pair = jnp.dot(normed[...], both, preferred_element_type=jnp.float32)
            out[:, here] = act(pair[:, :rest], pair[:, rest:]).astype(out.dtype)
        else:
            out[:, here] = act(product(left, here), product(right, here)).astype(out.dtype)


def terms_kernel(slots, parts, low, cores, far, whose, where, inside, hidden, *refs):
    shards = refs[: slots * parts]
    outs = refs[slots * parts : slots * parts + cores]
    columns, sems = refs[slots * parts + cores :]
    depth, width = shards[0].shape[0], columns.shape[2]

    def wanted(slot):
        return where[slot] > 0 if far else where[slot] == 0

    for slot in range(slots):

        @pl.when(wanted(slot))
        def _(slot=slot):
            for part in range(parts):
                pltpu.make_async_copy(
                    shards[part * slots + slot].at[:, pl.ds(low, width)],
                    columns.at[slot, pl.ds(part * depth, depth), :],
                    sems.at[part, slot],
                ).start()

    @pl.loop(0, slots)
    def _(slot):
        @pl.when(wanted(slot))
        def _():
            for part in range(parts):
                landing = columns.at[slot, pl.ds(part * depth, depth), :]
                pltpu.make_async_copy(landing, landing, sems.at[part, slot]).wait()
            value = jnp.dot(hidden[...], columns[slot], preferred_element_type=jnp.float32)
            value = value.astype(jnp.bfloat16)
            here = pl.ds(pl.multiple_of(inside[slot] * width, width), width)
            to = where[slot] - 1 if far else 0
            for core in range(cores):

                @pl.when(whose[slot] == core)
                def _(core=core):
                    outs[core][to, :, here] = value


def silu_times(gate, up):
    return gate / (1.0 + jnp.exp(-gate)) * up


def gate_times(gate, value):
    return value / (1.0 + jnp.exp(-gate))


class Ring:
    def __init__(self, order):
        count = len(order)
        after = {order[i]: order[(i + 1) % count] for i in range(count)}
        self.count = count
        self.forward = sorted(after.items())
        self.backward = sorted((b, a) for a, b in after.items())
        owners = np.zeros((count, count), np.int32)
        for place, index in enumerate(order):
            owners[index] = [order[(place + offset) % count] for offset in range(count)]
        row = lax.dynamic_slice_in_dim(jnp.asarray(owners), lax.axis_index("fs"), 1, axis=0)
        self.owners = row[0]


class Gathered:
    def __init__(self, ring, shard, onward):
        self.ring, self.onward = ring, onward
        self.ahead = self.behind = shard
        self.step = 0
        self.shards = {0: shard}

    def steps(self):
        return self.ring.count // 2

    def complete(self):
        return len(self.shards) == self.ring.count

    def ways(self):
        if self.step < self.ring.count - self.step:
            return (True, False)
        return (self.onward,)

    def sends(self):
        self.step += 1
        return [
            (self.ahead, self.ring.forward) if onward else (self.behind, self.ring.backward)
            for onward in self.ways()
        ]

    def accept(self, landed):
        for onward in self.ways():
            shard = landed.pop(0)
            if onward:
                self.ahead = shard
                self.shards[self.ring.count - self.step] = shard
            else:
                self.behind = shard
                self.shards[self.step] = shard

    def listed(self):
        return [self.shards[offset] for offset in range(self.ring.count)]


GATE_ONE, UP_ONE, DOWN_ONE, MIX, GATE_TWO, UP_TWO, DOWN_TWO, DOWN_MORE = range(8)


def order_of(steps):
    order = [GATE_ONE, UP_ONE] * steps + [DOWN_ONE, MIX] * steps
    late = [DOWN_TWO, DOWN_MORE] * steps
    for left in reversed(range(steps)):
        order += [GATE_TWO, UP_TWO]
        order += [late.pop(0) for _ in range(2 if left == 1 else min(left, 1))]
    return order + late


def may_launch(waiting, flying, depth):
    return bool(waiting) and len(flying) < depth and waiting[0] not in flying


class Pump:
    def __init__(self, groups, order, depth):
        self.groups, self.depth = groups, depth
        self.waiting = list(order)
        self.flying = []
        self.sent = 0
        self.mark = lax.axis_index("fs")

    def launch(self, value):
        key = self.waiting.pop(0)
        sends = [send for item in self.groups[key] for send in item.sends()]
        arrays, value = tie([array for array, _ in sends], value)
        landed = [lax.ppermute(a, "fs", way) for a, (_, way) in zip(arrays, sends)]
        self.flying.append((key, landed, self.sent))
        self.sent += 1
        return value

    def fill(self, value):
        while may_launch(self.waiting, [key for key, _, _ in self.flying], self.depth):
            value = self.launch(value)
        return value

    def until(self, items, value):
        while not all(item.complete() for item in items):
            value = self.turn(value)
        return value

    def turn(self, value, times=1):
        for _ in range(times):
            if not self.flying:
                return value
            key, landed, _ = self.flying.pop(0)
            landed, self.mark, value = tie(landed, self.mark, value)
            landed = list(landed)
            for item in self.groups[key]:
                item.accept(landed)
            self.mark, value = self.fill((self.mark, value))
            if self.flying:
                self.mark = self.mark + 1
                self.mark, value = tie(self.mark, value)
        return value


class Features:
    def __init__(self, count, cores):
        self.count, self.cores, self.chips = count, cores, count // cores
        index = lax.axis_index("tp")
        self.chip, self.core = index // cores, index % cores

    def across_core(self, value, shift):
        pairs = [
            (y * self.cores + c, y * self.cores + (c + shift) % self.cores)
            for y in range(self.chips)
            for c in range(self.cores)
        ]
        return lax.ppermute(value, "tp", pairs)

    def across_chip(self, value, shift):
        pairs = [
            (y * self.cores + c, (y + shift) % self.chips * self.cores + c)
            for y in range(self.chips)
            for c in range(self.cores)
        ]
        return lax.ppermute(value, "tp", pairs)

    def place_of(self, chip_shift, core_shift):
        chip = (self.chip - chip_shift + self.chips) % self.chips
        core = (self.core - core_shift + self.cores) % self.cores
        return chip * self.cores + core

    def gather_far(self, mine):
        return [self.across_chip(mine, shift) for shift in range(1, self.chips)]

    def gather_near(self, far):
        return [
            self.across_core(piece, shift) if shift else piece
            for piece in far
            for shift in range(self.cores)
        ]

    def blocks(self):
        return jnp.stack(
            [
                (self.chip - chip + self.chips) % self.chips * self.cores
                + (self.core - core + self.cores) % self.cores
                for chip in range(self.chips)
                for core in range(self.cores)
            ]
        )

    def spots(self, owners, each):
        holder = owners // each
        chip = (self.chip - holder // self.cores + self.chips) % self.chips
        core = (self.core - holder % self.cores + self.cores) % self.cores
        return (chip * self.cores + core) * each + owners % each

    def targets(self, owners, each):
        holder = owners // each
        chip = (holder // self.cores - self.chip + self.chips) % self.chips
        core = (holder % self.cores - self.core + self.cores) % self.cores
        return core, chip, owners % each

    def over_cores(self, terms):
        sent = [self.across_core(part, shift) for shift, part in enumerate(terms[1:], 1)]
        total = terms[0].astype(jnp.float32)
        for part in sent:
            total = total + part.astype(jnp.float32)
        return total

    def over_chips(self, sums):
        sums = sums.astype(jnp.bfloat16)
        return [self.across_chip(sums[shift - 1], shift) for shift in range(1, self.chips)]


def add_up(current, own, landed, factor):
    total = own[0]
    for part in landed:
        total = total + part.astype(jnp.float32)
    return (current.astype(jnp.float32) + factor * total).astype(jnp.bfloat16)


def solution(mesh):
    order = grid_ring(mesh)
    cores = cores_of(mesh)
    depth = 3

    def per_device(
        tokens,
        ffn_one_gain,
        ffn_one_gate,
        ffn_one_up,
        ffn_one_down,
        mix_gain,
        conv_value,
        conv_gate,
        conv_kernel,
        conv_ln_gain,
        conv_out,
        ffn_two_gain,
        ffn_two_gate,
        ffn_two_up,
        ffn_two_down,
    ):
        ring = Ring(order)
        features = Features(lax.axis_size("tp"), cores)
        channels = conv_ln_gain.shape[0] * lax.axis_size("tp")
        wide = conv_value.shape[1]
        half = ffn_two_down.shape[0] // 2
        one_gate = Gathered(ring, ffn_one_gate, True)
        one_up = Gathered(ring, ffn_one_up, False)
        one_down = Gathered(ring, ffn_one_down, True)
        if conv_value.shape[0] == conv_out.shape[0]:
            mixed = jnp.concatenate([conv_value, conv_gate, conv_out], axis=1)
            mix_in = mix_out = Gathered(ring, mixed, False)
            mixes, out_from = [mix_in], 2 * wide
        else:
            mix_in = Gathered(ring, jnp.concatenate([conv_value, conv_gate], axis=1), False)
            mix_out, out_from = Gathered(ring, conv_out, False), 0
            mixes = [mix_in, mix_out]
        two_gate = Gathered(ring, ffn_two_gate, True)
        two_up = Gathered(ring, ffn_two_up, False)
        two_down = [
            Gathered(ring, ffn_two_down[:half], True),
            Gathered(ring, ffn_two_down[half:], False),
        ]
        groups = {
            GATE_ONE: [one_gate],
            UP_ONE: [one_up],
            DOWN_ONE: [one_down],
            MIX: mixes,
            GATE_TWO: [two_gate],
            UP_TWO: [two_up],
            DOWN_TWO: [two_down[0]],
            DOWN_MORE: [two_down[1]],
        }
        pump = Pump(groups, order_of(ring.count // 2), depth)

        count = features.count
        each = ring.count // count
        blocks = features.blocks()
        spots = features.spots(ring.owners, each)
        targets = features.targets(ring.owners, each)
        vmem, smem, hbm = pltpu.VMEM, pltpu.SMEM, pltpu.HBM

        def hidden_of(parts, gain_vec, sides, lanes, width, act, dtype):
            length, size = parts[0].shape
            rows = count * size
            arrays = [shard for side in sides for shard in side.listed()]
            return pl.pallas_call(
                lambda *refs: hidden_kernel(
                    count, ring.count, len(sides), lanes, act, *refs
                ),
                out_shape=jax.ShapeDtypeStruct((length, width), dtype),
                in_specs=[spec(smem)] * 2 + [spec(vmem)] * (1 + count) + [spec(hbm)] * len(arrays),
                out_specs=spec(vmem),
                scratch_shapes=[
                    pltpu.VMEM((length, rows), jnp.bfloat16),
                    pltpu.VMEM((rows, width), jnp.bfloat16),
                    pltpu.VMEM((rows, width), jnp.bfloat16),
                    pltpu.SemaphoreType.DMA((2, ring.count)),
                ],
                cost_estimate=pl.CostEstimate(
                    flops=4 * length * rows * width,
                    bytes_accessed=4 * rows * width + 2 * length * rows,
                    transcendentals=length * width,
                ),
                name="hidden",
            )(spots, blocks, gain_vec.reshape(count, 1, size), *parts, *arrays)

        def terms_of(hidden, sides, low, width, far):
            length, depth_all = hidden.shape
            arrays = [shard for side in sides for shard in side.listed()]
            chips = features.chips - 1 if far else 1
            out = jax.ShapeDtypeStruct((chips, length, each * width), jnp.bfloat16)
            return pl.pallas_call(
                lambda *refs: terms_kernel(ring.count, len(sides), low, cores, far, *refs),
                out_shape=[out] * cores,
                in_specs=[spec(smem)] * 3 + [spec(vmem)] + [spec(hbm)] * len(arrays),
                out_specs=[spec(vmem)] * cores,
                scratch_shapes=[
                    pltpu.VMEM((ring.count, depth_all, width), jnp.bfloat16),
                    pltpu.SemaphoreType.DMA((len(sides), ring.count)),
                ],
                cost_estimate=pl.CostEstimate(
                    flops=2 * length * depth_all * chips * cores * each * width,
                    bytes_accessed=2 * depth_all * chips * cores * each * width,
                    transcendentals=0,
                ),
                name="far_terms" if far else "near_terms",
            )(*targets, hidden, *arrays)

        def scatter(hidden, sides, low, width, turns):
            landed = []
            if features.chips > 1:
                sums = features.over_cores(terms_of(hidden, sides, low, width, True))
                hidden, sums = tie(hidden, sums)
                landed = features.over_chips(sums)
            terms = terms_of(hidden, sides, low, width, False)
            own = features.over_cores(terms)
            return pump.turn(own, turns), landed

        tokens = pump.fill(tokens)
        far = features.gather_far(tokens)
        far = pump.turn(far)
        parts = features.gather_near([tokens] + far)
        parts = pump.until([one_gate, one_up], parts)
        hidden = hidden_of(
            parts, ffn_one_gain, [one_gate, one_up], (0, 0), ffn_one_up.shape[1], silu_times,
            jnp.bfloat16,
        )
        hidden = pump.until([one_down] + mixes, hidden)
        own, landed = scatter(hidden, [one_down], 0, ffn_one_down.shape[1], 1)
        stream_one = add_up(tokens, own, landed, 0.5)

        far = features.gather_far(stream_one)
        stream_one = pump.turn(stream_one, 2)
        parts = features.gather_near([stream_one] + far)
        gated_lin = hidden_of(
            parts, mix_gain, [mix_in], (wide, 0), wide, gate_times, jnp.float32
        )
        half_span = conv_kernel.shape[0] // 2
        convolved = lax.conv_general_dilated(
            gated_lin[None],
            conv_kernel[:, None, :],
            (1,),
            [(half_span, half_span)],
            dimension_numbers=("NWC", "WIO", "NWC"),
            feature_group_count=gated_lin.shape[1],
            precision=lax.Precision.HIGHEST,
        )[0]
        convolved = pump.turn(convolved, 2)
        sum_one, sum_two = lax.psum(
            (jnp.sum(convolved, axis=1), jnp.sum(convolved * convolved, axis=1)), "tp"
        )
        mean_val = (sum_one / channels)[:, None]
        varied = (sum_two / channels)[:, None] - mean_val * mean_val
        active = jax.nn.silu(
            (convolved - mean_val) * lax.rsqrt(varied + 1e-05) * conv_ln_gain
        ).astype(jnp.bfloat16)
        active = pump.turn(active)
        own, landed = scatter(active, [mix_out], out_from, conv_out.shape[1], 1)
        stream_two = add_up(stream_one, own, landed, 1.0)

        far = features.gather_far(stream_two)
        stream_two = pump.turn(stream_two, 3)
        parts = features.gather_near([stream_two] + far)
        parts = pump.until([two_gate, two_up], parts)
        hidden = hidden_of(
            parts, ffn_two_gain, [two_gate, two_up], (0, 0), ffn_two_up.shape[1], silu_times,
            jnp.bfloat16,
        )
        hidden = pump.until(two_down, hidden)
        own, landed = scatter(hidden, two_down, 0, ffn_two_down.shape[1], 0)
        return jnp.where(pump.mark < 0, stream_two, add_up(stream_two, own, landed, 0.5))

    in_specs = (
        P("fs", "tp"),
        P(),
        P("fs", "tp"),
        P("fs", "tp"),
        P("tp", "fs"),
        P(),
        P("fs", "tp"),
        P("fs", "tp"),
        P(None, "tp"),
        P("tp"),
        P("tp", "fs"),
        P(),
        P("fs", "tp"),
        P("fs", "tp"),
        P("tp", "fs"),
    )
    return jax.shard_map(
        per_device, mesh=mesh, in_specs=in_specs, out_specs=P("fs", "tp"), check_vma=False
    )
```

```python
import jax
import jax.numpy as jnp
import numpy as np
from jax import lax
from jax.experimental import pallas as pl
from jax.experimental.pallas import tpu as pltpu
from jax.sharding import PartitionSpec as P


def spots_of(devices):
    return [tuple(getattr(device, "coords", (0, 0, place))) for place, device in enumerate(devices)]


def grid_ring(mesh):
    count = mesh.shape["fs"]
    spots = spots_of(mesh.devices.reshape(count, -1)[:, 0])
    xs = sorted({spot[0] for spot in spots})
    zs = sorted({spot[2] for spot in spots})
    if len(xs) < 2 or len(zs) % 2 or len(xs) * len(zs) != count:
        return list(range(count))
    where = {(spot[0], spot[2]): index for index, spot in enumerate(spots)}
    walk = [(xs[0], z) for z in zs]
    for turn, z in enumerate(reversed(zs)):
        inner = xs[1:] if turn % 2 == 0 else xs[:0:-1]
        walk += [(x, z) for x in inner]
    return [where[spot] for spot in walk]


def cores_of(mesh):
    spots = spots_of(mesh.devices.reshape(-1, mesh.shape["tp"])[0])
    cores = sum(spot == spots[0] for spot in spots)
    return cores if mesh.shape["tp"] % cores == 0 else 1


def tie(*values):
    return lax.optimization_barrier(values)


def spec(space):
    return pl.BlockSpec(memory_space=space)


def hidden_kernel(blocks, rows, sides, lanes, act, spots, turn, gain, *refs):
    tokens = refs[:blocks]
    shards = [refs[blocks + i * rows : blocks + (i + 1) * rows] for i in range(sides)]
    out, normed, left, right, sems = refs[blocks + sides * rows :]
    depth = shards[0][0].shape[0]
    width = left.shape[1]
    tile = 256
    whole_tiles = width // tile
    cut = (whole_tiles + 1) // 2 * tile

    def copies_of(chunk, low, length):
        copies = []
        for which, whole in enumerate((left, right)):
            source = shards[which % sides]
            for slot in range(rows):
                at = pl.multiple_of(spots[slot] * depth, depth)
                copies.append(
                    pltpu.make_async_copy(
                        source[slot].at[:, pl.ds(lanes[which] + low, length)],
                        whole.at[pl.ds(at, depth), pl.ds(low, length)],
                        sems.at[chunk, which, slot],
                    )
                )
        return copies

    chunks = [
        copies_of(chunk, low, length)
        for chunk, (low, length) in enumerate([(0, cut), (cut, width - cut)])
        if length
    ]
    for copies in chunks:
        for copy in copies:
            copy.start()

    count, size = tokens[0].shape
    step = 64 if count % 64 == 0 else count

    @pl.loop(0, count // step)
    def _(index):
        here = pl.ds(pl.multiple_of(index * step, step), step)
        parts = [token[here, :].astype(jnp.float32) for token in tokens]
        total = sum(jnp.sum(part * part, axis=1, keepdims=True) for part in parts)
        scale = lax.rsqrt(total / (size * blocks) + 1e-06)
        for place_at, part in enumerate(parts):
            scaled = part * scale * gain[turn[place_at]]
            normed[here, place_at * size : (place_at + 1) * size] = scaled.astype(jnp.bfloat16)

    def product(whole, here):
        return jnp.dot(normed[...], whole[:, here], preferred_element_type=jnp.float32)

    for chunk, copies in enumerate(chunks):
        for copy in copies:
            copy.wait()

        @pl.loop(*((0, cut // tile) if chunk == 0 else (cut // tile, whole_tiles)))
        def _(index):
            here = pl.ds(pl.multiple_of(index * tile, tile), tile)
            out[:, here] = act(product(left, here), product(right, here)).astype(out.dtype)

    rest = width - whole_tiles * tile
    if rest:
        here = pl.ds(whole_tiles * tile, rest)
        if rest % 128 == 0:
            both = jnp.concatenate([left[:, here], right[:, here]], axis=1)
            pair = jnp.dot(normed[...], both, preferred_element_type=jnp.float32)
            out[:, here] = act(pair[:, :rest], pair[:, rest:]).astype(out.dtype)
        else:
            out[:, here] = act(product(left, here), product(right, here)).astype(out.dtype)


ALL, EARLY, LAST = range(3)


def terms_kernel(slots, parts, low, cores, far, when, whose, where, inside, hidden, *refs):
    last = slots // 2
    used = [slot for slot in range(slots) if when == ALL or (slot == last) == (when == LAST)]
    shards = refs[: len(used) * parts]
    outs = refs[len(used) * parts : len(used) * parts + cores]
    columns, sems = refs[len(used) * parts + cores :]
    width = columns.shape[2]
    depths = [shards[part * len(used)].shape[0] for part in range(parts)]
    spans = [(sum(depths[:part]), depths[part]) for part in range(parts)]

    def wanted(slot):
        return where[slot] > 0 if far else where[slot] == 0

    def put(slot, value):
        first = 0 if when == LAST else pl.multiple_of(inside[slot] * width, width)
        to = where[slot] - 1 if far else 0
        for core in range(cores):

            @pl.when(whose[slot] == core)
            def _(core=core):
                outs[core][to, :, pl.ds(first, width)] = value

    for number, slot in enumerate(used):

        @pl.when(wanted(slot))
        def _(number=number, slot=slot):
            for part in range(parts):
                pltpu.make_async_copy(
                    shards[part * len(used) + number].at[:, pl.ds(low, width)],
                    columns.at[slot, pl.ds(*spans[part]), :],
                    sems.at[part, slot],
                ).start()

    def product(slot):
        for part in range(parts):
            landing = columns.at[slot, pl.ds(*spans[part]), :]
            pltpu.make_async_copy(landing, landing, sems.at[part, slot]).wait()
        value = jnp.dot(hidden[...], columns[slot], preferred_element_type=jnp.float32)
        put(slot, value.astype(jnp.bfloat16))

    if when == LAST:
        for out in outs:
            out[...] = jnp.zeros_like(out)
        pl.when(wanted(last))(lambda: product(last))
        return
    if when == EARLY:
        empty = jnp.zeros((hidden.shape[0], width), jnp.bfloat16)
        pl.when(wanted(last))(lambda: put(last, empty))

    @pl.loop(0, slots)
    def _(slot):
        here = wanted(slot)
        if when == EARLY:
            here = jnp.logical_and(here, slot != last)
        pl.when(here)(lambda: product(slot))


def silu_times(gate, up):
    return gate / (1.0 + jnp.exp(-gate)) * up


def gate_times(gate, value):
    return value / (1.0 + jnp.exp(-gate))


class Ring:
    def __init__(self, order):
        count = len(order)
        after = {order[i]: order[(i + 1) % count] for i in range(count)}
        self.count = count
        self.forward = sorted(after.items())
        self.backward = sorted((b, a) for a, b in after.items())
        owners = np.zeros((count, count), np.int32)
        for place, index in enumerate(order):
            owners[index] = [order[(place + offset) % count] for offset in range(count)]
        row = lax.dynamic_slice_in_dim(jnp.asarray(owners), lax.axis_index("fs"), 1, axis=0)
        self.owners = row[0]


class Gathered:
    def __init__(self, ring, shard, onward):
        self.ring, self.onward = ring, onward
        self.ahead = self.behind = shard
        self.step = 0
        self.shards = {0: shard}

    def steps(self):
        return self.ring.count // 2

    def complete(self):
        return len(self.shards) == self.ring.count

    def ways(self):
        if self.step < self.ring.count - self.step:
            return (True, False)
        return (self.onward,)

    def sends(self):
        self.step += 1
        return [
            (self.ahead, self.ring.forward) if onward else (self.behind, self.ring.backward)
            for onward in self.ways()
        ]

    def accept(self, landed):
        for onward in self.ways():
            shard = landed.pop(0)
            if onward:
                self.ahead = shard
                self.shards[self.ring.count - self.step] = shard
            else:
                self.behind = shard
                self.shards[self.step] = shard

    def nearly(self):
        return len(self.shards) >= self.ring.count - 1

    def listed(self):
        return [self.shards[offset] for offset in range(self.ring.count)]


GATE_ONE, UP_ONE, DOWN_ONE, MIX, GATE_TWO, UP_TWO, DOWN_TWO, DOWN_MORE = range(8)


def order_of(steps):
    order = [GATE_ONE, UP_ONE] * steps + [DOWN_ONE, MIX] * steps
    late = [DOWN_TWO, DOWN_MORE] * steps
    for left in reversed(range(steps)):
        order += [GATE_TWO, UP_TWO]
        order += [late.pop(0) for _ in range(2 if left == 1 else min(left, 1))]
    return order + late


def may_launch(waiting, flying, depth):
    return bool(waiting) and len(flying) < depth and waiting[0] not in flying


class Pump:
    def __init__(self, groups, order, depth):
        self.groups, self.depth = groups, depth
        self.waiting = list(order)
        self.flying = []
        self.sent = 0
        self.mark = lax.axis_index("fs")

    def launch(self, value):
        key = self.waiting.pop(0)
        sends = [send for item in self.groups[key] for send in item.sends()]
        arrays, value = tie([array for array, _ in sends], value)
        landed = [lax.ppermute(a, "fs", way) for a, (_, way) in zip(arrays, sends)]
        self.flying.append((key, landed, self.sent))
        self.sent += 1
        return value

    def fill(self, value):
        while may_launch(self.waiting, [key for key, _, _ in self.flying], self.depth):
            value = self.launch(value)
        return value

    def until(self, items, value):
        while not all(item.complete() for item in items):
            value = self.turn(value)
        return value

    def until_nearly(self, items, value):
        while not all(item.nearly() for item in items):
            value = self.turn(value)
        return value

    def turn(self, value, times=1):
        for _ in range(times):
            if not self.flying:
                return value
            key, landed, _ = self.flying.pop(0)
            landed, self.mark, value = tie(landed, self.mark, value)
            landed = list(landed)
            for item in self.groups[key]:
                item.accept(landed)
            self.mark, value = self.fill((self.mark, value))
            if self.flying:
                self.mark = self.mark + 1
                self.mark, value = tie(self.mark, value)
        return value


class Features:
    def __init__(self, count, cores):
        self.count, self.cores, self.chips = count, cores, count // cores
        index = lax.axis_index("tp")
        self.chip, self.core = index // cores, index % cores

    def across_core(self, value, shift):
        pairs = [
            (y * self.cores + c, y * self.cores + (c + shift) % self.cores)
            for y in range(self.chips)
            for c in range(self.cores)
        ]
        return lax.ppermute(value, "tp", pairs)

    def across_chip(self, value, shift):
        pairs = [
            (y * self.cores + c, (y + shift) % self.chips * self.cores + c)
            for y in range(self.chips)
            for c in range(self.cores)
        ]
        return lax.ppermute(value, "tp", pairs)

    def place_of(self, chip_shift, core_shift):
        chip = (self.chip - chip_shift + self.chips) % self.chips
        core = (self.core - core_shift + self.cores) % self.cores
        return chip * self.cores + core

    def gather_far(self, mine):
        return [self.across_chip(mine, shift) for shift in range(1, self.chips)]

    def gather_near(self, far):
        return [
            self.across_core(piece, shift) if shift else piece
            for piece in far
            for shift in range(self.cores)
        ]

    def blocks(self):
        return jnp.stack(
            [
                (self.chip - chip + self.chips) % self.chips * self.cores
                + (self.core - core + self.cores) % self.cores
                for chip in range(self.chips)
                for core in range(self.cores)
            ]
        )

    def spots(self, owners, each):
        holder = owners // each
        chip = (self.chip - holder // self.cores + self.chips) % self.chips
        core = (self.core - holder % self.cores + self.cores) % self.cores
        return (chip * self.cores + core) * each + owners % each

    def targets(self, owners, each):
        holder = owners // each
        chip = (holder // self.cores - self.chip + self.chips) % self.chips
        core = (holder % self.cores - self.core + self.cores) % self.cores
        return core, chip, owners % each

    def over_cores(self, terms):
        sent = [self.across_core(part, shift) for shift, part in enumerate(terms[1:], 1)]
        total = terms[0].astype(jnp.float32)
        for part in sent:
            total = total + part.astype(jnp.float32)
        return total

    def over_chips(self, sums):
        sums = sums.astype(jnp.bfloat16)
        return [self.across_chip(sums[shift - 1], shift) for shift in range(1, self.chips)]


def add_up(current, sums, factor):
    totals = []
    for own, landed in sums:
        total = own[0]
        for part in landed:
            total = total + part.astype(jnp.float32)
        totals.append(total)
    total = jnp.concatenate(totals, axis=0) if len(totals) > 1 else totals[0]
    return (current.astype(jnp.float32) + factor * total).astype(jnp.bfloat16)


def solution(mesh):
    order = grid_ring(mesh)
    cores = cores_of(mesh)
    depth = 3

    def per_device(
        tokens,
        ffn_one_gain,
        ffn_one_gate,
        ffn_one_up,
        ffn_one_down,
        mix_gain,
        conv_value,
        conv_gate,
        conv_kernel,
        conv_ln_gain,
        conv_out,
        ffn_two_gain,
        ffn_two_gate,
        ffn_two_up,
        ffn_two_down,
    ):
        ring = Ring(order)
        features = Features(lax.axis_size("tp"), cores)
        channels = conv_ln_gain.shape[0] * lax.axis_size("tp")
        wide = conv_value.shape[1]
        half = ffn_two_down.shape[0] // 2
        one_gate = Gathered(ring, ffn_one_gate, True)
        one_up = Gathered(ring, ffn_one_up, False)
        cut = conv_value.size + conv_gate.size + conv_out.size + ffn_one_down.size
        cut = cut // (2 * ffn_one_down.shape[1]) // 16 * 16
        one_down = [
            Gathered(ring, ffn_one_down[:cut], True),
            Gathered(ring, ffn_one_down[cut:], False),
        ]
        if conv_value.shape[0] == conv_out.shape[0]:
            mixed = jnp.concatenate([conv_value, conv_gate, conv_out], axis=1)
            mix_in = mix_out = Gathered(ring, mixed, False)
            mixes, out_from = [mix_in], 2 * wide
        else:
            mix_in = Gathered(ring, jnp.concatenate([conv_value, conv_gate], axis=1), False)
            mix_out, out_from = Gathered(ring, conv_out, False), 0
            mixes = [mix_in, mix_out]
        two_gate = Gathered(ring, ffn_two_gate, True)
        two_up = Gathered(ring, ffn_two_up, False)
        two_down = [
            Gathered(ring, ffn_two_down[:half], True),
            Gathered(ring, ffn_two_down[half:], False),
        ]
        groups = {
            GATE_ONE: [one_gate],
            UP_ONE: [one_up],
            DOWN_ONE: one_down,
            MIX: mixes,
            GATE_TWO: [two_gate],
            UP_TWO: [two_up],
            DOWN_TWO: [two_down[0]],
            DOWN_MORE: [two_down[1]],
        }
        pump = Pump(groups, order_of(ring.count // 2), depth)

        count = features.count
        each = ring.count // count
        blocks = features.blocks()
        spots = features.spots(ring.owners, each)
        targets = features.targets(ring.owners, each)
        vmem, smem, hbm = pltpu.VMEM, pltpu.SMEM, pltpu.HBM

        def hidden_of(parts, gain_vec, sides, lanes, width, act, dtype):
            size = parts[0].shape[1]
            length = parts[0].shape[0]
            rows = count * size
            arrays = [shard for side in sides for shard in side.listed()]
            return pl.pallas_call(
                lambda *refs: hidden_kernel(
                    count, ring.count, len(sides), lanes, act, *refs
                ),
                out_shape=jax.ShapeDtypeStruct((length, width), dtype),
                in_specs=[spec(smem)] * 2
                + [spec(vmem)]
                + [spec(vmem)] * count
                + [spec(hbm)] * len(arrays),
                out_specs=spec(vmem),
                scratch_shapes=[
                    pltpu.VMEM((length, rows), jnp.bfloat16),
                    pltpu.VMEM((rows, width), jnp.bfloat16),
                    pltpu.VMEM((rows, width), jnp.bfloat16),
                    pltpu.SemaphoreType.DMA((2, 2, ring.count)),
                ],
                cost_estimate=pl.CostEstimate(
                    flops=4 * length * rows * width,
                    bytes_accessed=4 * rows * width + 2 * length * rows,
                    transcendentals=length * width,
                ),
                name="hidden",
            )(spots, blocks, gain_vec.reshape(count, 1, size), *parts, *arrays)

        def terms_of(hidden, sides, low, width, far, when=ALL):
            length, depth_all = hidden.shape
            last = ring.count // 2
            arrays = [
                side.shards[slot]
                for side in sides
                for slot in range(ring.count)
                if when == ALL or (slot == last) == (when == LAST)
            ]
            chips = features.chips - 1 if far else 1
            wide_out = width if when == LAST else each * width
            out = jax.ShapeDtypeStruct((chips, length, wide_out), jnp.bfloat16)
            return pl.pallas_call(
                lambda *refs: terms_kernel(
                    ring.count, len(sides), low, cores, far, when, *refs
                ),
                out_shape=[out] * cores,
                in_specs=[spec(smem)] * 3 + [spec(vmem)] + [spec(hbm)] * len(arrays),
                out_specs=[spec(vmem)] * cores,
                scratch_shapes=[
                    pltpu.VMEM((ring.count, depth_all, width), jnp.bfloat16),
                    pltpu.SemaphoreType.DMA((len(sides), ring.count)),
                ],
                cost_estimate=pl.CostEstimate(
                    flops=2 * length * depth_all * chips * cores * each * width,
                    bytes_accessed=2 * depth_all * chips * cores * each * width,
                    transcendentals=0,
                ),
                name="far_terms" if far else "near_terms",
            )(*targets, hidden, *arrays)

        def far_in_two(hidden, sides, low, width):
            hidden = pump.until_nearly(sides, hidden)
            early = features.over_cores(terms_of(hidden, sides, low, width, True, EARLY))
            hidden, early = pump.until(sides, (hidden, early))
            late = features.over_cores(terms_of(hidden, sides, low, width, True, LAST))
            spot = targets[2][ring.count // 2]
            spread = [jnp.where(spot == place_at, late, 0.0) for place_at in range(each)]
            return hidden, early + jnp.concatenate(spread, axis=-1)

        def scatter(hiddens, sides, low, width, turns, waits=False):
            landed = [[] for _ in hiddens]
            hiddens = list(hiddens)
            if features.chips > 1:
                for number in reversed(range(len(hiddens))):
                    if waits:
                        hiddens[number], sums = far_in_two(hiddens[number], sides, low, width)
                    else:
                        terms = terms_of(hiddens[number], sides, low, width, True)
                        sums = features.over_cores(terms)
                    hiddens, sums = tie(hiddens, sums.astype(jnp.bfloat16))
                    landed[number] = features.over_chips(sums)
            owns = []
            for hidden in hiddens:
                terms = terms_of(hidden, sides, low, width, False)
                owns.append(features.over_cores(terms))
            return list(zip(pump.turn(owns, turns), landed))

        tokens = pump.fill(tokens)
        far = features.gather_far(tokens)
        far = pump.turn(far)
        parts = features.gather_near([tokens] + far)
        parts = pump.until([one_gate, one_up], parts)
        hidden = hidden_of(
            parts, ffn_one_gain, [one_gate, one_up], (0, 0), ffn_one_up.shape[1], silu_times,
            jnp.bfloat16,
        )
        hidden = pump.until(one_down + mixes, hidden)
        sums = scatter([hidden], one_down, 0, ffn_one_down.shape[1], 1)
        stream_one = add_up(tokens, sums, 0.5)

        far = features.gather_far(stream_one)
        stream_one = pump.turn(stream_one, 2)
        parts = features.gather_near([stream_one] + far)
        gated_lin = hidden_of(
            parts, mix_gain, [mix_in], (wide, 0), wide, gate_times, jnp.float32
        )
        half_span = conv_kernel.shape[0] // 2
        convolved = lax.conv_general_dilated(
            gated_lin[None],
            conv_kernel[:, None, :],
            (1,),
            [(half_span, half_span)],
            dimension_numbers=("NWC", "WIO", "NWC"),
            feature_group_count=gated_lin.shape[1],
            precision=lax.Precision.HIGHEST,
        )[0]
        convolved = pump.turn(convolved, 2)
        sum_one, sum_two = lax.psum(
            (jnp.sum(convolved, axis=1), jnp.sum(convolved * convolved, axis=1)), "tp"
        )
        mean_val = (sum_one / channels)[:, None]
        varied = (sum_two / channels)[:, None] - mean_val * mean_val
        active = jax.nn.silu(
            (convolved - mean_val) * lax.rsqrt(varied + 1e-05) * conv_ln_gain
        ).astype(jnp.bfloat16)
        active = pump.turn(active)
        sums = scatter([active], [mix_out], out_from, conv_out.shape[1], 1)
        stream_two = add_up(stream_one, sums, 1.0)

        far = features.gather_far(stream_two)
        stream_two = pump.turn(stream_two, 3)
        parts = features.gather_near([stream_two] + far)
        parts = pump.until([two_gate, two_up], parts)
        hidden = hidden_of(
            parts, ffn_two_gain, [two_gate, two_up], (0, 0), ffn_two_up.shape[1], silu_times,
            jnp.bfloat16,
        )
        waits = features.chips > 1 and ring.count % 2 == 0
        if not waits:
            hidden = pump.until(two_down, hidden)
        sums = scatter([hidden], two_down, 0, ffn_two_down.shape[1], 0, waits)
        return jnp.where(pump.mark < 0, stream_two, add_up(stream_two, sums, 0.5))

    in_specs = (
        P("fs", "tp"),
        P(),
        P("fs", "tp"),
        P("fs", "tp"),
        P("tp", "fs"),
        P(),
        P("fs", "tp"),
        P("fs", "tp"),
        P(None, "tp"),
        P("tp"),
        P("tp", "fs"),
        P(),
        P("fs", "tp"),
        P("fs", "tp"),
        P("tp", "fs"),
    )
    return jax.shard_map(
        per_device, mesh=mesh, in_specs=in_specs, out_specs=P("fs", "tp"), check_vma=False
    )
```

```python
import jax
import jax.numpy as jnp
import numpy as np
from jax import lax
from jax.experimental import pallas as pl
from jax.experimental.pallas import tpu as pltpu
from jax.sharding import PartitionSpec as P


def spots_of(devices):
    return [tuple(getattr(device, "coords", (0, 0, place))) for place, device in enumerate(devices)]


def grid_ring(mesh):
    count = mesh.shape["fs"]
    spots = spots_of(mesh.devices.reshape(count, -1)[:, 0])
    xs = sorted({spot[0] for spot in spots})
    zs = sorted({spot[2] for spot in spots})
    if len(xs) < 2 or len(zs) % 2 or len(xs) * len(zs) != count:
        return list(range(count))
    where = {(spot[0], spot[2]): index for index, spot in enumerate(spots)}
    walk = [(xs[0], z) for z in zs]
    for turn, z in enumerate(reversed(zs)):
        inner = xs[1:] if turn % 2 == 0 else xs[:0:-1]
        walk += [(x, z) for x in inner]
    return [where[spot] for spot in walk]


def cores_of(mesh):
    spots = spots_of(mesh.devices.reshape(-1, mesh.shape["tp"])[0])
    cores = sum(spot == spots[0] for spot in spots)
    return cores if mesh.shape["tp"] % cores == 0 else 1


def tie(*values):
    return lax.optimization_barrier(values)


def spec(space):
    return pl.BlockSpec(memory_space=space)


def hidden_kernel(blocks, rows, sides, lanes, act, spots, turn, gain, *refs):
    tokens = refs[:blocks]
    shards = [refs[blocks + i * rows : blocks + (i + 1) * rows] for i in range(sides)]
    out, normed, left, right, sems = refs[blocks + sides * rows :]
    depth = shards[0][0].shape[0]
    width = left.shape[1]
    tile = 256
    whole_tiles = width // tile
    cut = (whole_tiles + 1) // 2 * tile

    def copies_of(chunk, low, length):
        copies = []
        for which, whole in enumerate((left, right)):
            source = shards[which % sides]
            for slot in range(rows):
                at = pl.multiple_of(spots[slot] * depth, depth)
                copies.append(
                    pltpu.make_async_copy(
                        source[slot].at[:, pl.ds(lanes[which] + low, length)],
                        whole.at[pl.ds(at, depth), pl.ds(low, length)],
                        sems.at[chunk, which, slot],
                    )
                )
        return copies

    chunks = [
        copies_of(chunk, low, length)
        for chunk, (low, length) in enumerate([(0, cut), (cut, width - cut)])
        if length
    ]
    for copies in chunks:
        for copy in copies:
            copy.start()

    count, size = tokens[0].shape
    step = 64 if count % 64 == 0 else count

    @pl.loop(0, count // step)
    def _(index):
        here = pl.ds(pl.multiple_of(index * step, step), step)
        parts = [token[here, :].astype(jnp.float32) for token in tokens]
        total = sum(jnp.sum(part * part, axis=1, keepdims=True) for part in parts)
        scale = lax.rsqrt(total / (size * blocks) + 1e-06)
        for place_at, part in enumerate(parts):
            scaled = part * scale * gain[turn[place_at]]
            normed[here, place_at * size : (place_at + 1) * size] = scaled.astype(jnp.bfloat16)

    def product(whole, here):
        return jnp.dot(normed[...], whole[:, here], preferred_element_type=jnp.float32)

    for chunk, copies in enumerate(chunks):
        for copy in copies:
            copy.wait()

        @pl.loop(*((0, cut // tile) if chunk == 0 else (cut // tile, whole_tiles)))
        def _(index):
            here = pl.ds(pl.multiple_of(index * tile, tile), tile)
            out[:, here] = act(product(left, here), product(right, here)).astype(out.dtype)

    rest = width - whole_tiles * tile
    if rest:
        here = pl.ds(whole_tiles * tile, rest)
        if rest % 128 == 0:
            both = jnp.concatenate([left[:, here], right[:, here]], axis=1)
            pair = jnp.dot(normed[...], both, preferred_element_type=jnp.float32)
            out[:, here] = act(pair[:, :rest], pair[:, rest:]).astype(out.dtype)
        else:
            out[:, here] = act(product(left, here), product(right, here)).astype(out.dtype)


ALL, EARLY, LAST = range(3)


def terms_kernel(slots, parts, low, cores, far, when, whose, where, inside, hidden, *refs):
    last = slots // 2
    used = [slot for slot in range(slots) if when == ALL or (slot == last) == (when == LAST)]
    shards = refs[: len(used) * parts]
    outs = refs[len(used) * parts : len(used) * parts + cores]
    columns, sems = refs[len(used) * parts + cores :]
    width = columns.shape[2]
    depths = [shards[part * len(used)].shape[0] for part in range(parts)]
    spans = [(sum(depths[:part]), depths[part]) for part in range(parts)]

    def wanted(slot):
        return where[slot] > 0 if far else where[slot] == 0

    def put(slot, value):
        first = 0 if when == LAST else pl.multiple_of(inside[slot] * width, width)
        to = where[slot] - 1 if far else 0
        for core in range(cores):

            @pl.when(whose[slot] == core)
            def _(core=core):
                outs[core][to, :, pl.ds(first, width)] = value

    for number, slot in enumerate(used):

        @pl.when(wanted(slot))
        def _(number=number, slot=slot):
            for part in range(parts):
                pltpu.make_async_copy(
                    shards[part * len(used) + number].at[:, pl.ds(low, width)],
                    columns.at[slot, pl.ds(*spans[part]), :],
                    sems.at[part, slot],
                ).start()

    def product(slot):
        for part in range(parts):
            landing = columns.at[slot, pl.ds(*spans[part]), :]
            pltpu.make_async_copy(landing, landing, sems.at[part, slot]).wait()
        value = jnp.dot(hidden[...], columns[slot], preferred_element_type=jnp.float32)
        put(slot, value.astype(jnp.bfloat16))

    if when == LAST:
        for out in outs:
            out[...] = jnp.zeros_like(out)
        pl.when(wanted(last))(lambda: product(last))
        return
    if when == EARLY:
        empty = jnp.zeros((hidden.shape[0], width), jnp.bfloat16)
        pl.when(wanted(last))(lambda: put(last, empty))

    @pl.loop(0, slots)
    def _(slot):
        here = wanted(slot)
        if when == EARLY:
            here = jnp.logical_and(here, slot != last)
        pl.when(here)(lambda: product(slot))


def silu_times(gate, up):
    return gate / (1.0 + jnp.exp(-gate)) * up


def gate_times(gate, value):
    return value / (1.0 + jnp.exp(-gate))


class Ring:
    def __init__(self, order):
        count = len(order)
        after = {order[i]: order[(i + 1) % count] for i in range(count)}
        self.count = count
        self.forward = sorted(after.items())
        self.backward = sorted((b, a) for a, b in after.items())
        owners = np.zeros((count, count), np.int32)
        for place, index in enumerate(order):
            owners[index] = [order[(place + offset) % count] for offset in range(count)]
        row = lax.dynamic_slice_in_dim(jnp.asarray(owners), lax.axis_index("fs"), 1, axis=0)
        self.owners = row[0]


class Gathered:
    def __init__(self, ring, shard, onward):
        self.ring, self.onward = ring, onward
        self.ahead = self.behind = shard
        self.step = 0
        self.shards = {0: shard}

    def steps(self):
        return self.ring.count // 2

    def complete(self):
        return len(self.shards) == self.ring.count

    def ways(self):
        if self.step < self.ring.count - self.step:
            return (True, False)
        return (self.onward,)

    def sends(self):
        self.step += 1
        return [
            (self.ahead, self.ring.forward) if onward else (self.behind, self.ring.backward)
            for onward in self.ways()
        ]

    def accept(self, landed):
        for onward in self.ways():
            shard = landed.pop(0)
            if onward:
                self.ahead = shard
                self.shards[self.ring.count - self.step] = shard
            else:
                self.behind = shard
                self.shards[self.step] = shard

    def nearly(self):
        return len(self.shards) >= self.ring.count - 1

    def listed(self):
        return [self.shards[offset] for offset in range(self.ring.count)]


GATE_ONE, UP_ONE, DOWN_ONE, MIX, GATE_TWO, UP_TWO, DOWN_TWO, DOWN_MORE = range(8)


def order_of(steps):
    order = [GATE_ONE, UP_ONE] * steps + [DOWN_ONE, MIX] * steps
    late = [DOWN_TWO, DOWN_MORE] * steps
    for left in reversed(range(steps)):
        order += [GATE_TWO, UP_TWO]
        order += [late.pop(0) for _ in range(2 if left == 1 else min(left, 1))]
    return order + late


def may_launch(waiting, flying, depth):
    return bool(waiting) and len(flying) < depth and waiting[0] not in flying


class Pump:
    def __init__(self, groups, order, depth):
        self.groups, self.depth = groups, depth
        self.waiting = list(order)
        self.flying = []
        self.sent = 0
        self.mark = lax.axis_index("fs")

    def launch(self, value):
        key = self.waiting.pop(0)
        sends = [send for item in self.groups[key] for send in item.sends()]
        arrays, value = tie([array for array, _ in sends], value)
        landed = [lax.ppermute(a, "fs", way) for a, (_, way) in zip(arrays, sends)]
        self.flying.append((key, landed, self.sent))
        self.sent += 1
        return value

    def fill(self, value):
        while may_launch(self.waiting, [key for key, _, _ in self.flying], self.depth):
            value = self.launch(value)
        return value

    def until(self, items, value):
        while not all(item.complete() for item in items):
            value = self.turn(value)
        return value

    def until_nearly(self, items, value):
        while not all(item.nearly() for item in items):
            value = self.turn(value)
        return value

    def turn(self, value, times=1):
        for _ in range(times):
            if not self.flying:
                return value
            key, landed, _ = self.flying.pop(0)
            landed, self.mark, value = tie(landed, self.mark, value)
            landed = list(landed)
            for item in self.groups[key]:
                item.accept(landed)
            self.mark, value = self.fill((self.mark, value))
            if self.flying:
                self.mark = self.mark + 1
                self.mark, value = tie(self.mark, value)
        return value


class Features:
    def __init__(self, count, cores):
        self.count, self.cores, self.chips = count, cores, count // cores
        index = lax.axis_index("tp")
        self.chip, self.core = index // cores, index % cores

    def across_core(self, value, shift):
        pairs = [
            (y * self.cores + c, y * self.cores + (c + shift) % self.cores)
            for y in range(self.chips)
            for c in range(self.cores)
        ]
        return lax.ppermute(value, "tp", pairs)

    def across_chip(self, value, shift):
        pairs = [
            (y * self.cores + c, (y + shift) % self.chips * self.cores + c)
            for y in range(self.chips)
            for c in range(self.cores)
        ]
        return lax.ppermute(value, "tp", pairs)

    def place_of(self, chip_shift, core_shift):
        chip = (self.chip - chip_shift + self.chips) % self.chips
        core = (self.core - core_shift + self.cores) % self.cores
        return chip * self.cores + core

    def gather_far(self, mine):
        return [self.across_chip(mine, shift) for shift in range(1, self.chips)]

    def gather_near(self, far):
        return [
            self.across_core(piece, shift) if shift else piece
            for piece in far
            for shift in range(self.cores)
        ]

    def blocks(self):
        return jnp.stack(
            [
                (self.chip - chip + self.chips) % self.chips * self.cores
                + (self.core - core + self.cores) % self.cores
                for chip in range(self.chips)
                for core in range(self.cores)
            ]
        )

    def spots(self, owners, each):
        holder = owners // each
        chip = (self.chip - holder // self.cores + self.chips) % self.chips
        core = (self.core - holder % self.cores + self.cores) % self.cores
        return (chip * self.cores + core) * each + owners % each

    def targets(self, owners, each):
        holder = owners // each
        chip = (holder // self.cores - self.chip + self.chips) % self.chips
        core = (holder % self.cores - self.core + self.cores) % self.cores
        return core, chip, owners % each

    def over_cores(self, terms):
        sent = [self.across_core(part, shift) for shift, part in enumerate(terms[1:], 1)]
        total = terms[0].astype(jnp.float32)
        for part in sent:
            total = total + part.astype(jnp.float32)
        return total

    def over_chips(self, sums):
        sums = sums.astype(jnp.bfloat16)
        return [self.across_chip(sums[shift - 1], shift) for shift in range(1, self.chips)]


def add_up(current, sums, factor):
    totals = []
    for own, landed in sums:
        total = own[0]
        for part in landed:
            total = total + part.astype(jnp.float32)
        totals.append(total)
    total = jnp.concatenate(totals, axis=0) if len(totals) > 1 else totals[0]
    return (current.astype(jnp.float32) + factor * total).astype(jnp.bfloat16)


def solution(mesh):
    order = grid_ring(mesh)
    cores = cores_of(mesh)
    depth = 3

    def per_device(
        tokens,
        ffn_one_gain,
        ffn_one_gate,
        ffn_one_up,
        ffn_one_down,
        mix_gain,
        conv_value,
        conv_gate,
        conv_kernel,
        conv_ln_gain,
        conv_out,
        ffn_two_gain,
        ffn_two_gate,
        ffn_two_up,
        ffn_two_down,
    ):
        ring = Ring(order)
        features = Features(lax.axis_size("tp"), cores)
        channels = conv_ln_gain.shape[0] * lax.axis_size("tp")
        wide = conv_value.shape[1]
        half = ffn_two_down.shape[0] // 2
        one_gate = Gathered(ring, ffn_one_gate, True)
        one_up = Gathered(ring, ffn_one_up, False)
        cut = conv_value.size + conv_gate.size + conv_out.size + ffn_one_down.size
        cut = cut // (2 * ffn_one_down.shape[1]) // 16 * 16
        one_down = [
            Gathered(ring, ffn_one_down[:cut], True),
            Gathered(ring, ffn_one_down[cut:], False),
        ]
        if conv_value.shape[0] == conv_out.shape[0]:
            mixed = jnp.concatenate([conv_value, conv_gate, conv_out], axis=1)
            mix_in = mix_out = Gathered(ring, mixed, False)
            mixes, out_from = [mix_in], 2 * wide
        else:
            mix_in = Gathered(ring, jnp.concatenate([conv_value, conv_gate], axis=1), False)
            mix_out, out_from = Gathered(ring, conv_out, False), 0
            mixes = [mix_in, mix_out]
        two_gate = Gathered(ring, ffn_two_gate, True)
        two_up = Gathered(ring, ffn_two_up, False)
        two_down = [
            Gathered(ring, ffn_two_down[:half], True),
            Gathered(ring, ffn_two_down[half:], False),
        ]
        groups = {
            GATE_ONE: [one_gate],
            UP_ONE: [one_up],
            DOWN_ONE: one_down,
            MIX: mixes,
            GATE_TWO: [two_gate],
            UP_TWO: [two_up],
            DOWN_TWO: [two_down[0]],
            DOWN_MORE: [two_down[1]],
        }
        pump = Pump(groups, order_of(ring.count // 2), depth)

        count = features.count
        each = ring.count // count
        blocks = features.blocks()
        spots = features.spots(ring.owners, each)
        targets = features.targets(ring.owners, each)
        vmem, smem, hbm = pltpu.VMEM, pltpu.SMEM, pltpu.HBM

        def hidden_of(parts, gain_vec, sides, lanes, width, act, dtype):
            size = parts[0].shape[1]
            length = parts[0].shape[0]
            rows = count * size
            arrays = [shard for side in sides for shard in side.listed()]
            return pl.pallas_call(
                lambda *refs: hidden_kernel(
                    count, ring.count, len(sides), lanes, act, *refs
                ),
                out_shape=jax.ShapeDtypeStruct((length, width), dtype),
                in_specs=[spec(smem)] * 2
                + [spec(vmem)]
                + [spec(vmem)] * count
                + [spec(hbm)] * len(arrays),
                out_specs=spec(vmem),
                scratch_shapes=[
                    pltpu.VMEM((length, rows), jnp.bfloat16),
                    pltpu.VMEM((rows, width), jnp.bfloat16),
                    pltpu.VMEM((rows, width), jnp.bfloat16),
                    pltpu.SemaphoreType.DMA((2, 2, ring.count)),
                ],
                cost_estimate=pl.CostEstimate(
                    flops=4 * length * rows * width,
                    bytes_accessed=4 * rows * width + 2 * length * rows,
                    transcendentals=length * width,
                ),
                name="hidden",
            )(spots, blocks, gain_vec.reshape(count, 1, size), *parts, *arrays)

        def terms_of(hidden, sides, low, width, far, when=ALL):
            length, depth_all = hidden.shape
            last = ring.count // 2
            arrays = [
                side.shards[slot]
                for side in sides
                for slot in range(ring.count)
                if when == ALL or (slot == last) == (when == LAST)
            ]
            chips = features.chips - 1 if far else 1
            wide_out = width if when == LAST else each * width
            out = jax.ShapeDtypeStruct((chips, length, wide_out), jnp.bfloat16)
            return pl.pallas_call(
                lambda *refs: terms_kernel(
                    ring.count, len(sides), low, cores, far, when, *refs
                ),
                out_shape=[out] * cores,
                in_specs=[spec(smem)] * 3 + [spec(vmem)] + [spec(hbm)] * len(arrays),
                out_specs=[spec(vmem)] * cores,
                scratch_shapes=[
                    pltpu.VMEM((ring.count, depth_all, width), jnp.bfloat16),
                    pltpu.SemaphoreType.DMA((len(sides), ring.count)),
                ],
                cost_estimate=pl.CostEstimate(
                    flops=2 * length * depth_all * chips * cores * each * width,
                    bytes_accessed=2 * depth_all * chips * cores * each * width,
                    transcendentals=0,
                ),
                name="far_terms" if far else "near_terms",
            )(*targets, hidden, *arrays)

        def far_in_two(hidden, sides, low, width):
            hidden = pump.until_nearly(sides, hidden)
            early = terms_of(hidden, sides, low, width, True, EARLY)
            hidden, early = pump.until(sides, (hidden, early))
            early = features.over_cores(early)
            late = terms_of(hidden, sides, low, width, True, LAST)
            late = features.over_cores(late)
            spot = targets[2][ring.count // 2]
            spread = [jnp.where(spot == place_at, late, 0.0) for place_at in range(each)]
            return hidden, early + jnp.concatenate(spread, axis=-1)

        def scatter(hiddens, sides, low, width, turns, waits=False):
            landed = [[] for _ in hiddens]
            hiddens = list(hiddens)
            if features.chips > 1:
                for number in reversed(range(len(hiddens))):
                    if waits:
                        hiddens[number], sums = far_in_two(hiddens[number], sides, low, width)
                    else:
                        terms = terms_of(hiddens[number], sides, low, width, True)
                        sums = features.over_cores(terms)
                    hiddens, sums = tie(hiddens, sums.astype(jnp.bfloat16))
                    landed[number] = features.over_chips(sums)
            owns = []
            for hidden in hiddens:
                terms = terms_of(hidden, sides, low, width, False)
                owns.append(features.over_cores(terms))
            return list(zip(pump.turn(owns, turns), landed))

        tokens = pump.fill(tokens)
        far = features.gather_far(tokens)
        far = pump.turn(far)
        parts = features.gather_near([tokens] + far)
        parts = pump.until([one_gate, one_up], parts)
        hidden = hidden_of(
            parts, ffn_one_gain, [one_gate, one_up], (0, 0), ffn_one_up.shape[1], silu_times,
            jnp.bfloat16,
        )
        hidden = pump.until(one_down + mixes, hidden)
        sums = scatter([hidden], one_down, 0, ffn_one_down.shape[1], 1)
        stream_one = add_up(tokens, sums, 0.5)

        far = features.gather_far(stream_one)
        stream_one = pump.turn(stream_one, 2)
        parts = features.gather_near([stream_one] + far)
        gated_lin = hidden_of(
            parts, mix_gain, [mix_in], (wide, 0), wide, gate_times, jnp.float32
        )
        half_span = conv_kernel.shape[0] // 2
        convolved = lax.conv_general_dilated(
            gated_lin[None],
            conv_kernel[:, None, :],
            (1,),
            [(half_span, half_span)],
            dimension_numbers=("NWC", "WIO", "NWC"),
            feature_group_count=gated_lin.shape[1],
            precision=lax.Precision.HIGHEST,
        )[0]
        convolved = pump.turn(convolved, 2)
        sum_one, sum_two = lax.psum(
            (jnp.sum(convolved, axis=1), jnp.sum(convolved * convolved, axis=1)), "tp"
        )
        mean_val = (sum_one / channels)[:, None]
        varied = (sum_two / channels)[:, None] - mean_val * mean_val
        active = jax.nn.silu(
            (convolved - mean_val) * lax.rsqrt(varied + 1e-05) * conv_ln_gain
        ).astype(jnp.bfloat16)
        active = pump.turn(active)
        sums = scatter([active], [mix_out], out_from, conv_out.shape[1], 1)
        stream_two = add_up(stream_one, sums, 1.0)

        far = features.gather_far(stream_two)
        stream_two = pump.turn(stream_two, 3)
        parts = features.gather_near([stream_two] + far)
        parts = pump.until([two_gate, two_up], parts)
        hidden = hidden_of(
            parts, ffn_two_gain, [two_gate, two_up], (0, 0), ffn_two_up.shape[1], silu_times,
            jnp.bfloat16,
        )
        waits = features.chips > 1 and ring.count % 2 == 0
        if not waits:
            hidden = pump.until(two_down, hidden)
        sums = scatter([hidden], two_down, 0, ffn_two_down.shape[1], 0, waits)
        return jnp.where(pump.mark < 0, stream_two, add_up(stream_two, sums, 0.5))

    in_specs = (
        P("fs", "tp"),
        P(),
        P("fs", "tp"),
        P("fs", "tp"),
        P("tp", "fs"),
        P(),
        P("fs", "tp"),
        P("fs", "tp"),
        P(None, "tp"),
        P("tp"),
        P("tp", "fs"),
        P(),
        P("fs", "tp"),
        P("fs", "tp"),
        P("tp", "fs"),
    )
    return jax.shard_map(
        per_device, mesh=mesh, in_specs=in_specs, out_specs=P("fs", "tp"), check_vma=False
    )
```

```python
import jax
import jax.numpy as jnp
import numpy as np
from jax import lax
from jax.experimental import pallas as pl
from jax.experimental.pallas import tpu as pltpu
from jax.sharding import PartitionSpec as P


def spots_of(devices):
    return [tuple(getattr(device, "coords", (0, 0, place))) for place, device in enumerate(devices)]


def grid_ring(mesh):
    count = mesh.shape["fs"]
    spots = spots_of(mesh.devices.reshape(count, -1)[:, 0])
    xs = sorted({spot[0] for spot in spots})
    zs = sorted({spot[2] for spot in spots})
    if len(xs) < 2 or len(zs) % 2 or len(xs) * len(zs) != count:
        return list(range(count))
    where = {(spot[0], spot[2]): index for index, spot in enumerate(spots)}
    walk = [(xs[0], z) for z in zs]
    for turn, z in enumerate(reversed(zs)):
        inner = xs[1:] if turn % 2 == 0 else xs[:0:-1]
        walk += [(x, z) for x in inner]
    return [where[spot] for spot in walk]


def cores_of(mesh):
    spots = spots_of(mesh.devices.reshape(-1, mesh.shape["tp"])[0])
    cores = sum(spot == spots[0] for spot in spots)
    return cores if mesh.shape["tp"] % cores == 0 else 1


def tie(*values):
    return lax.optimization_barrier(values)


def spec(space):
    return pl.BlockSpec(memory_space=space)


def hidden_kernel(blocks, rows, sides, lanes, act, spots, turn, gain, *refs):
    tokens = refs[:blocks]
    shards = [refs[blocks + i * rows : blocks + (i + 1) * rows] for i in range(sides)]
    out, normed, left, right, sems = refs[blocks + sides * rows :]
    depth = shards[0][0].shape[0]
    width = left.shape[1]
    tile = 256
    whole_tiles = width // tile
    cut = (whole_tiles + 1) // 2 * tile

    def copies_of(chunk, low, length):
        copies = []
        for which, whole in enumerate((left, right)):
            source = shards[which % sides]
            for slot in range(rows):
                at = pl.multiple_of(spots[slot] * depth, depth)
                copies.append(
                    pltpu.make_async_copy(
                        source[slot].at[:, pl.ds(lanes[which] + low, length)],
                        whole.at[pl.ds(at, depth), pl.ds(low, length)],
                        sems.at[chunk, which, slot],
                    )
                )
        return copies

    chunks = [
        copies_of(chunk, low, length)
        for chunk, (low, length) in enumerate([(0, cut), (cut, width - cut)])
        if length
    ]
    for copies in chunks:
        for copy in copies:
            copy.start()

    count, size = tokens[0].shape
    step = 64 if count % 64 == 0 else count

    @pl.loop(0, count // step)
    def _(index):
        here = pl.ds(pl.multiple_of(index * step, step), step)
        parts = [token[here, :].astype(jnp.float32) for token in tokens]
        total = sum(jnp.sum(part * part, axis=1, keepdims=True) for part in parts)
        scale = lax.rsqrt(total / (size * blocks) + 1e-06)
        for place_at, part in enumerate(parts):
            scaled = part * scale * gain[turn[place_at]]
            normed[here, place_at * size : (place_at + 1) * size] = scaled.astype(jnp.bfloat16)

    def product(whole, here):
        return jnp.dot(normed[...], whole[:, here], preferred_element_type=jnp.float32)

    for chunk, copies in enumerate(chunks):
        for copy in copies:
            copy.wait()

        @pl.loop(*((0, cut // tile) if chunk == 0 else (cut // tile, whole_tiles)))
        def _(index):
            here = pl.ds(pl.multiple_of(index * tile, tile), tile)
            out[:, here] = act(product(left, here), product(right, here)).astype(out.dtype)

    rest = width - whole_tiles * tile
    if rest:
        here = pl.ds(whole_tiles * tile, rest)
        if rest % 128 == 0:
            both = jnp.concatenate([left[:, here], right[:, here]], axis=1)
            pair = jnp.dot(normed[...], both, preferred_element_type=jnp.float32)
            out[:, here] = act(pair[:, :rest], pair[:, rest:]).astype(out.dtype)
        else:
            out[:, here] = act(product(left, here), product(right, here)).astype(out.dtype)


ALL, EARLY, LAST = range(3)


def terms_kernel(slots, parts, low, cores, far, when, whose, where, inside, hidden, *refs):
    last = slots // 2
    used = [slot for slot in range(slots) if when == ALL or (slot == last) == (when == LAST)]
    shards = refs[: len(used) * parts]
    outs = refs[len(used) * parts : len(used) * parts + cores]
    columns, sems = refs[len(used) * parts + cores :]
    width = columns.shape[2]
    depths = [shards[part * len(used)].shape[0] for part in range(parts)]
    spans = [(sum(depths[:part]), depths[part]) for part in range(parts)]

    def wanted(slot):
        return where[slot] > 0 if far else where[slot] == 0

    def put(slot, value):
        first = 0 if when == LAST else pl.multiple_of(inside[slot] * width, width)
        to = where[slot] - 1 if far else 0
        for core in range(cores):

            @pl.when(whose[slot] == core)
            def _(core=core):
                outs[core][to, :, pl.ds(first, width)] = value

    if when == LAST:
        for out in outs:
            out[...] = jnp.zeros_like(out)

        @pl.when(wanted(last))
        def _():
            for part, shard in enumerate(shards):
                columns[0, pl.ds(*spans[part]), :] = shard[:, low : low + width]
            value = jnp.dot(hidden[...], columns[0], preferred_element_type=jnp.float32)
            put(last, value.astype(jnp.bfloat16))

        return

    for number, slot in enumerate(used):

        @pl.when(wanted(slot))
        def _(number=number, slot=slot):
            for part in range(parts):
                pltpu.make_async_copy(
                    shards[part * len(used) + number].at[:, pl.ds(low, width)],
                    columns.at[slot, pl.ds(*spans[part]), :],
                    sems.at[part, slot],
                ).start()

    def product(slot):
        for part in range(parts):
            landing = columns.at[slot, pl.ds(*spans[part]), :]
            pltpu.make_async_copy(landing, landing, sems.at[part, slot]).wait()
        value = jnp.dot(hidden[...], columns[slot], preferred_element_type=jnp.float32)
        put(slot, value.astype(jnp.bfloat16))

    if when == EARLY:
        empty = jnp.zeros((hidden.shape[0], width), jnp.bfloat16)
        pl.when(wanted(last))(lambda: put(last, empty))

    @pl.loop(0, slots)
    def _(slot):
        here = wanted(slot)
        if when == EARLY:
            here = jnp.logical_and(here, slot != last)
        pl.when(here)(lambda: product(slot))


def silu_times(gate, up):
    return gate / (1.0 + jnp.exp(-gate)) * up


def gate_times(gate, value):
    return value / (1.0 + jnp.exp(-gate))


class Ring:
    def __init__(self, order):
        count = len(order)
        after = {order[i]: order[(i + 1) % count] for i in range(count)}
        self.count = count
        self.forward = sorted(after.items())
        self.backward = sorted((b, a) for a, b in after.items())
        owners = np.zeros((count, count), np.int32)
        for place, index in enumerate(order):
            owners[index] = [order[(place + offset) % count] for offset in range(count)]
        row = lax.dynamic_slice_in_dim(jnp.asarray(owners), lax.axis_index("fs"), 1, axis=0)
        self.owners = row[0]


class Gathered:
    def __init__(self, ring, shard, onward):
        self.ring, self.onward = ring, onward
        self.ahead = self.behind = shard
        self.step = 0
        self.shards = {0: shard}

    def steps(self):
        return self.ring.count // 2

    def complete(self):
        return len(self.shards) == self.ring.count

    def ways(self):
        if self.step < self.ring.count - self.step:
            return (True, False)
        return (self.onward,)

    def sends(self):
        self.step += 1
        return [
            (self.ahead, self.ring.forward) if onward else (self.behind, self.ring.backward)
            for onward in self.ways()
        ]

    def accept(self, landed):
        for onward in self.ways():
            shard = landed.pop(0)
            if onward:
                self.ahead = shard
                self.shards[self.ring.count - self.step] = shard
            else:
                self.behind = shard
                self.shards[self.step] = shard

    def nearly(self):
        return len(self.shards) >= self.ring.count - 1

    def listed(self):
        return [self.shards[offset] for offset in range(self.ring.count)]


GATE_ONE, UP_ONE, DOWN_ONE, MIX, GATE_TWO, UP_TWO, DOWN_TWO, DOWN_MORE = range(8)


def order_of(steps):
    order = [GATE_ONE, UP_ONE] * steps + [DOWN_ONE, MIX] * steps
    late = [DOWN_TWO, DOWN_MORE] * steps
    for left in reversed(range(steps)):
        order += [GATE_TWO, UP_TWO]
        order += [late.pop(0) for _ in range(2 if left == 1 else min(left, 1))]
    return order + late


def may_launch(waiting, flying, depth):
    return bool(waiting) and len(flying) < depth and waiting[0] not in flying


class Pump:
    def __init__(self, groups, order, depth):
        self.groups, self.depth = groups, depth
        self.waiting = list(order)
        self.flying = []
        self.sent = 0
        self.mark = lax.axis_index("fs")

    def launch(self, value):
        key = self.waiting.pop(0)
        sends = [send for item in self.groups[key] for send in item.sends()]
        arrays, value = tie([array for array, _ in sends], value)
        landed = [lax.ppermute(a, "fs", way) for a, (_, way) in zip(arrays, sends)]
        self.flying.append((key, landed, self.sent))
        self.sent += 1
        return value

    def fill(self, value):
        while may_launch(self.waiting, [key for key, _, _ in self.flying], self.depth):
            value = self.launch(value)
        return value

    def until(self, items, value):
        while not all(item.complete() for item in items):
            value = self.turn(value)
        return value

    def until_nearly(self, items, value):
        while not all(item.nearly() for item in items):
            value = self.turn(value)
        return value

    def turn(self, value, times=1):
        for _ in range(times):
            if not self.flying:
                return value
            key, landed, _ = self.flying.pop(0)
            landed, self.mark, value = tie(landed, self.mark, value)
            landed = list(landed)
            for item in self.groups[key]:
                item.accept(landed)
            self.mark, value = self.fill((self.mark, value))
            if self.flying:
                self.mark = self.mark + 1
                self.mark, value = tie(self.mark, value)
        return value


class Features:
    def __init__(self, count, cores):
        self.count, self.cores, self.chips = count, cores, count // cores
        index = lax.axis_index("tp")
        self.chip, self.core = index // cores, index % cores

    def across_core(self, value, shift):
        pairs = [
            (y * self.cores + c, y * self.cores + (c + shift) % self.cores)
            for y in range(self.chips)
            for c in range(self.cores)
        ]
        return lax.ppermute(value, "tp", pairs)

    def across_chip(self, value, shift):
        pairs = [
            (y * self.cores + c, (y + shift) % self.chips * self.cores + c)
            for y in range(self.chips)
            for c in range(self.cores)
        ]
        return lax.ppermute(value, "tp", pairs)

    def place_of(self, chip_shift, core_shift):
        chip = (self.chip - chip_shift + self.chips) % self.chips
        core = (self.core - core_shift + self.cores) % self.cores
        return chip * self.cores + core

    def gather_far(self, mine):
        return [self.across_chip(mine, shift) for shift in range(1, self.chips)]

    def gather_near(self, far):
        return [
            self.across_core(piece, shift) if shift else piece
            for piece in far
            for shift in range(self.cores)
        ]

    def blocks(self):
        return jnp.stack(
            [
                (self.chip - chip + self.chips) % self.chips * self.cores
                + (self.core - core + self.cores) % self.cores
                for chip in range(self.chips)
                for core in range(self.cores)
            ]
        )

    def spots(self, owners, each):
        holder = owners // each
        chip = (self.chip - holder // self.cores + self.chips) % self.chips
        core = (self.core - holder % self.cores + self.cores) % self.cores
        return (chip * self.cores + core) * each + owners % each

    def targets(self, owners, each):
        holder = owners // each
        chip = (holder // self.cores - self.chip + self.chips) % self.chips
        core = (holder % self.cores - self.core + self.cores) % self.cores
        return core, chip, owners % each

    def over_cores(self, terms):
        sent = [self.across_core(part, shift) for shift, part in enumerate(terms[1:], 1)]
        total = terms[0].astype(jnp.float32)
        for part in sent:
            total = total + part.astype(jnp.float32)
        return total

    def over_chips(self, sums):
        sums = sums.astype(jnp.bfloat16)
        return [self.across_chip(sums[shift - 1], shift) for shift in range(1, self.chips)]


def add_up(current, sums, factor):
    totals = []
    for own, landed in sums:
        total = own[0]
        for part in landed:
            total = total + part.astype(jnp.float32)
        totals.append(total)
    total = jnp.concatenate(totals, axis=0) if len(totals) > 1 else totals[0]
    return (current.astype(jnp.float32) + factor * total).astype(jnp.bfloat16)


def solution(mesh):
    order = grid_ring(mesh)
    cores = cores_of(mesh)
    depth = 4

    def per_device(
        tokens,
        ffn_one_gain,
        ffn_one_gate,
        ffn_one_up,
        ffn_one_down,
        mix_gain,
        conv_value,
        conv_gate,
        conv_kernel,
        conv_ln_gain,
        conv_out,
        ffn_two_gain,
        ffn_two_gate,
        ffn_two_up,
        ffn_two_down,
    ):
        ring = Ring(order)
        features = Features(lax.axis_size("tp"), cores)
        channels = conv_ln_gain.shape[0] * lax.axis_size("tp")
        wide = conv_value.shape[1]
        half = ffn_two_down.shape[0] // 2
        one_gate = Gathered(ring, ffn_one_gate, True)
        one_up = Gathered(ring, ffn_one_up, False)
        cut = conv_value.size + conv_gate.size + conv_out.size + ffn_one_down.size
        cut = cut // (2 * ffn_one_down.shape[1]) // 16 * 16
        one_down = [
            Gathered(ring, ffn_one_down[:cut], True),
            Gathered(ring, ffn_one_down[cut:], False),
        ]
        if conv_value.shape[0] == conv_out.shape[0]:
            mixed = jnp.concatenate([conv_value, conv_gate, conv_out], axis=1)
            mix_in = mix_out = Gathered(ring, mixed, False)
            mixes, out_from = [mix_in], 2 * wide
        else:
            mix_in = Gathered(ring, jnp.concatenate([conv_value, conv_gate], axis=1), False)
            mix_out, out_from = Gathered(ring, conv_out, False), 0
            mixes = [mix_in, mix_out]
        two_gate = Gathered(ring, ffn_two_gate, True)
        two_up = Gathered(ring, ffn_two_up, False)
        two_down = [
            Gathered(ring, ffn_two_down[:half], True),
            Gathered(ring, ffn_two_down[half:], False),
        ]
        groups = {
            GATE_ONE: [one_gate],
            UP_ONE: [one_up],
            DOWN_ONE: one_down,
            MIX: mixes,
            GATE_TWO: [two_gate],
            UP_TWO: [two_up],
            DOWN_TWO: [two_down[0]],
            DOWN_MORE: [two_down[1]],
        }
        pump = Pump(groups, order_of(ring.count // 2), depth)

        count = features.count
        each = ring.count // count
        blocks = features.blocks()
        spots = features.spots(ring.owners, each)
        targets = features.targets(ring.owners, each)
        vmem, smem, hbm = pltpu.VMEM, pltpu.SMEM, pltpu.HBM

        def hidden_of(parts, gain_vec, sides, lanes, width, act, dtype):
            size = parts[0].shape[1]
            length = parts[0].shape[0]
            rows = count * size
            arrays = [shard for side in sides for shard in side.listed()]
            return pl.pallas_call(
                lambda *refs: hidden_kernel(
                    count, ring.count, len(sides), lanes, act, *refs
                ),
                out_shape=jax.ShapeDtypeStruct((length, width), dtype),
                in_specs=[spec(smem)] * 2
                + [spec(vmem)]
                + [spec(vmem)] * count
                + [spec(hbm)] * len(arrays),
                out_specs=spec(vmem),
                scratch_shapes=[
                    pltpu.VMEM((length, rows), jnp.bfloat16),
                    pltpu.VMEM((rows, width), jnp.bfloat16),
                    pltpu.VMEM((rows, width), jnp.bfloat16),
                    pltpu.SemaphoreType.DMA((2, 2, ring.count)),
                ],
                cost_estimate=pl.CostEstimate(
                    flops=4 * length * rows * width,
                    bytes_accessed=4 * rows * width + 2 * length * rows,
                    transcendentals=length * width,
                ),
                name="hidden",
            )(spots, blocks, gain_vec.reshape(count, 1, size), *parts, *arrays)

        def terms_of(hidden, sides, low, width, far, when=ALL):
            length, depth_all = hidden.shape
            last = ring.count // 2
            arrays = [
                side.shards[slot]
                for side in sides
                for slot in range(ring.count)
                if when == ALL or (slot == last) == (when == LAST)
            ]
            chips = features.chips - 1 if far else 1
            wide_out = width if when == LAST else each * width
            out = jax.ShapeDtypeStruct((chips, length, wide_out), jnp.bfloat16)
            return pl.pallas_call(
                lambda *refs: terms_kernel(
                    ring.count, len(sides), low, cores, far, when, *refs
                ),
                out_shape=[out] * cores,
                in_specs=[spec(smem)] * 3
                + [spec(vmem)]
                + [spec(vmem if when == LAST else hbm)] * len(arrays),
                out_specs=[spec(vmem)] * cores,
                scratch_shapes=[
                    pltpu.VMEM((1 if when == LAST else ring.count, depth_all, width), jnp.bfloat16),
                    pltpu.SemaphoreType.DMA((len(sides), ring.count)),
                ],
                cost_estimate=pl.CostEstimate(
                    flops=2 * length * depth_all * chips * cores * each * width,
                    bytes_accessed=2 * depth_all * chips * cores * each * width,
                    transcendentals=0,
                ),
                name="far_terms" if far else "near_terms",
            )(*targets, hidden, *arrays)

        def far_in_two(hidden, sides, low, width):
            hidden = pump.until_nearly(sides, hidden)
            early = terms_of(hidden, sides, low, width, True, EARLY)
            hidden, early = pump.until(sides, (hidden, early))
            early = features.over_cores(early)
            late = terms_of(hidden, sides, low, width, True, LAST)
            late = features.over_cores(late)
            spot = targets[2][ring.count // 2]
            spread = [jnp.where(spot == place_at, late, 0.0) for place_at in range(each)]
            return hidden, early + jnp.concatenate(spread, axis=-1)

        def scatter(hiddens, sides, low, width, turns, waits=False):
            landed = [[] for _ in hiddens]
            hiddens = list(hiddens)
            if features.chips > 1:
                for number in reversed(range(len(hiddens))):
                    if waits:
                        hiddens[number], sums = far_in_two(hiddens[number], sides, low, width)
                    else:
                        terms = terms_of(hiddens[number], sides, low, width, True)
                        sums = features.over_cores(terms)
                    hiddens, sums = tie(hiddens, sums.astype(jnp.bfloat16))
                    landed[number] = features.over_chips(sums)
            owns = []
            for hidden in hiddens:
                terms = terms_of(hidden, sides, low, width, False)
                owns.append(features.over_cores(terms))
            return list(zip(pump.turn(owns, turns), landed))

        tokens = pump.fill(tokens)
        far = features.gather_far(tokens)
        far = pump.turn(far)
        parts = features.gather_near([tokens] + far)
        parts = pump.until([one_gate, one_up], parts)
        hidden = hidden_of(
            parts, ffn_one_gain, [one_gate, one_up], (0, 0), ffn_one_up.shape[1], silu_times,
            jnp.bfloat16,
        )
        hidden = pump.until(one_down + mixes, hidden)
        sums = scatter([hidden], one_down, 0, ffn_one_down.shape[1], 1)
        stream_one = add_up(tokens, sums, 0.5)

        far = features.gather_far(stream_one)
        stream_one = pump.turn(stream_one, 2)
        parts = features.gather_near([stream_one] + far)
        gated_lin = hidden_of(
            parts, mix_gain, [mix_in], (wide, 0), wide, gate_times, jnp.float32
        )
        half_span = conv_kernel.shape[0] // 2
        convolved = lax.conv_general_dilated(
            gated_lin[None],
            conv_kernel[:, None, :],
            (1,),
            [(half_span, half_span)],
            dimension_numbers=("NWC", "WIO", "NWC"),
            feature_group_count=gated_lin.shape[1],
            precision=lax.Precision.HIGHEST,
        )[0]
        convolved = pump.turn(convolved, 2)
        sum_one, sum_two = lax.psum(
            (jnp.sum(convolved, axis=1), jnp.sum(convolved * convolved, axis=1)), "tp"
        )
        mean_val = (sum_one / channels)[:, None]
        varied = (sum_two / channels)[:, None] - mean_val * mean_val
        active = jax.nn.silu(
            (convolved - mean_val) * lax.rsqrt(varied + 1e-05) * conv_ln_gain
        ).astype(jnp.bfloat16)
        active = pump.turn(active)
        sums = scatter([active], [mix_out], out_from, conv_out.shape[1], 1)
        stream_two = add_up(stream_one, sums, 1.0)

        far = features.gather_far(stream_two)
        stream_two = pump.turn(stream_two, 3)
        parts = features.gather_near([stream_two] + far)
        parts = pump.until([two_gate, two_up], parts)
        hidden = hidden_of(
            parts, ffn_two_gain, [two_gate, two_up], (0, 0), ffn_two_up.shape[1], silu_times,
            jnp.bfloat16,
        )
        waits = features.chips > 1 and ring.count % 2 == 0
        if not waits:
            hidden = pump.until(two_down, hidden)
        sums = scatter([hidden], two_down, 0, ffn_two_down.shape[1], 0, waits)
        return jnp.where(pump.mark < 0, stream_two, add_up(stream_two, sums, 0.5))

    in_specs = (
        P("fs", "tp"),
        P(),
        P("fs", "tp"),
        P("fs", "tp"),
        P("tp", "fs"),
        P(),
        P("fs", "tp"),
        P("fs", "tp"),
        P(None, "tp"),
        P("tp"),
        P("tp", "fs"),
        P(),
        P("fs", "tp"),
        P("fs", "tp"),
        P("tp", "fs"),
    )
    return jax.shard_map(
        per_device, mesh=mesh, in_specs=in_specs, out_specs=P("fs", "tp"), check_vma=False
    )
```
